32 devices in a mesh: sp: 8 (over z, core), tp: 4 (over y, x).
Axes of the slice: x: 2, y: 2, z: 4, core: 2. Of those that a mesh axis runs over, the one named last changes fastest.
Arguments:
- pool_in: bfloat16 [512, 3072], P('tp', 'sp'), may hold values from -8 to 8
- doc_ids: int32 [3072], P('sp'), may hold values from 0 to 3, never falling along the last dimension, each value on 1 to 1536 neighbouring positions
- pool_map: bfloat16 [8, 64, 64], replicated, may hold values from -0.75 to 0.75
- pool_scale: float32 [512], replicated, may hold values from 0.1 to 1.9
- w_out: bfloat16 [512, 2048], P(None, 'tp'), may hold values from -0.25 to 0.25
- gate_logit: bfloat16 [3072, 2048], P('sp', 'tp'), may hold values from -8 to 8
- residual: bfloat16 [3072, 2048], P('sp', 'tp'), may hold values from -4 to 4
- first_gain: float32 [2048], P('tp'), may hold values from 0.1 to 1.9
- first_bias: float32 [2048], P('tp'), may hold values from -1.5 to 1.5
- routes: int32 [3072, 2], P('sp'), may hold values from 0 to 7, all different within a row; in each aligned block of 384 rows (0 to 383, 384 to 767, ...) at most 192 rows name the same one
- route_weight: float32 [3072, 2], P('sp'), may hold values from 0.25 to 1
- w_gate: bfloat16 [8, 2048, 1024], P('sp', None, 'tp'), may hold values from -0.125 to 0.125
- w_up: bfloat16 [8, 2048, 1024], P('sp', None, 'tp'), may hold values from -0.125 to 0.125
- w_down: bfloat16 [8, 1024, 2048], P('sp', None, 'tp'), may hold values from -0.375 to 0.375
- second_gain: float32 [2048], P('tp'), may hold values from 0.1 to 1.9
- second_bias: float32 [2048], P('tp'), may hold values from -1.5 to 1.5
Outputs:
- layer_out: bfloat16 [3072, 2048], P('sp', 'tp')
The draws below stay inside these ranges and needn't reach their ends.
Inputs may be any that keep to these rules, and one draw needn't show every extreme that they name: `doc_ids`: never falling; each document spans 1 to 1536 positions. `routes`: each row names 2 different experts; in each aligned block of 384 rows (the rows of one index of sp) no expert is named by more than 192 rows, a bound that some block reaches.
All inputs are finite; a program needn't handle non-finite values.
Results may differ from the reference program's by a relative error of at most 0.008.
Values may be sent and summed in bfloat16 or wider, within the bound.
No kernel may reach another device: no remote copies, remote signals or barrier semaphores. Data moves between devices by JAX's collectives and lax.ppermute only.
A program may use at most 64 MiB of HBM per device.

```python
import math
import jax
import jax.numpy as jnp
import numpy as np
from jax import lax

D = 2048
MIX_W = 512
GROUP_W = 64
GROUPS = 8
DE = 1024
TOPK = 2
TOK_DEV = 384
TOKENS = 3072
EXPERTS = 8
CAP = 192
DOCS = 4
DOC_MOST = 1536
N_SP = 8


def draw_pool_in(key, part):
    walk_key, rough_key = jax.random.split(jax.random.fold_in(key, 7))
    blocks = TOKENS // 16
    drift_walk = jnp.cumsum(jax.random.normal(walk_key, (MIX_W, blocks), jnp.float32), axis=1)
    drift_walk = drift_walk / jnp.sqrt(jnp.float32(blocks))
    smooth = jnp.repeat(drift_walk, 16, axis=1)
    rough_part = jax.random.normal(rough_key, (MIX_W, TOKENS), jnp.float32)
    return jnp.clip(0.8 * rough_part + smooth, -8.0, 8.0).astype(jnp.bfloat16)


def level_of(own_key, shape, shards, least, top_value):
    loudness = 1.0
    for dim, blocks in shards:
        steps = jax.random.uniform(jax.random.fold_in(jax.random.fold_in(own_key, 6), dim), (blocks,), jnp.float32, least / len(shards), top_value / len(shards))
        loudness = loudness * jnp.repeat(jnp.exp(steps), shape[dim] // blocks).reshape((-1,) + (1,) * (len(shape) - 1 - dim))
    return loudness


def length_profile(amount, total, limit, lean):
    portions = [(1 << 20) // math.isqrt(standing ** lean) + 1 for standing in range(2, amount + 1)]
    spare, holding = total - limit - (amount - 1), [1] * (amount - 1)
    while spare > 0:
        candidates = [i for i in range(amount - 1) if holding[i] < limit]
        whole, left = sum([portions[i] for i in candidates]), spare
        for i in candidates:
            addition = min(limit - holding[i], max(1, left * portions[i] // whole), spare)
            holding[i] = holding[i] + addition
            spare = spare - addition
    return np.array([limit] + holding)


def uneven(rng, number_of, total, bound, lean):
    if number_of == 2:
        one = jax.random.randint(rng, (), max(1, total - bound), min(bound, total - 1) + 1)
        return jnp.stack([one, total - one])
    lengths = jnp.asarray(length_profile(number_of, total, bound, lean), jnp.int32)
    twos = (number_of - 1) // 2
    giver, receiver = lengths[1:1 + 2 * twos:2], lengths[2:2 + 2 * twos:2]
    room = jnp.minimum(giver - 1, bound - receiver)
    passed = jax.random.randint(jax.random.fold_in(rng, 1), (twos,), 0, 1 << 20) % (room + 1)
    lengths = lengths.at[1:1 + 2 * twos:2].set(giver - passed).at[2:2 + 2 * twos:2].set(receiver + passed)
    return lengths[jax.random.permutation(jax.random.fold_in(rng, 2), number_of)]


def routed_block(stream_key, own, number, rows, amount, top, most, slope):
    order = jax.random.permutation(stream_key, amount)
    crowded, ordinary = portions_of(amount, rows * top, most, slope, True), portions_of(amount, rows * top, most, slope, False)
    places = jnp.arange(amount)

    def named(lengths, rotation):
        used = int((lengths > 0).sum())
        fixed = max(1, used // 4)
        shifted = fixed + (places - fixed + rotation * (used - fixed)) % max(1, amount - fixed)
        return jnp.zeros((amount,), jnp.int32).at[order[jnp.where(places < fixed, places, shifted)]].set(jnp.asarray(lengths, jnp.int32))

    lengths = jnp.where(number % 4 == 0, named(crowded, number // 4), named(ordinary, number - number // 4 - 1))
    mixed = jax.random.permutation(jax.random.fold_in(own, 3), amount)
    donor, receiver = mixed[0:amount // 2 * 2:2], mixed[1:amount // 2 * 2:2]
    slack = jnp.minimum(lengths[donor] - 1, most - lengths[receiver]) // 2
    slack = jnp.where((donor == order[0]) | (receiver == order[0]) | (lengths[receiver] == 0), 0, jnp.maximum(slack, 0))
    shifted = jax.random.randint(jax.random.fold_in(own, 4), (amount // 2,), 0, 1 << 20) % (slack + 1)
    lengths = lengths.at[donor].add(-shifted).at[receiver].add(shifted)
    labels = jnp.searchsorted(jnp.cumsum(lengths), jnp.arange(rows * top), side="right").astype(jnp.int32)
    grid = labels.reshape(top, rows).T
    grid = grid[jax.random.permutation(jax.random.fold_in(own, 1), rows)]
    rotation = jax.random.randint(jax.random.fold_in(own, 2), (rows, 1), 0, top)
    return jnp.take_along_axis(grid, (jnp.arange(top)[None, :] + rotation) % top, axis=1)


def portions_of(amount, total, limit, slope, full):
    loads = [(1 << 20) // math.isqrt(rank ** slope) + 1 for rank in range(1, amount + 1)]
    largest = limit if full else min(limit, max(-(-total // amount), total * loads[0] // sum(loads)))
    least = 1 if total - largest >= amount - 1 else 0
    holding, spare = [largest] + [least] * (amount - 1), total - largest - least * (amount - 1)
    while spare > 0:
        candidates = [i for i in range(1, amount) if holding[i] < largest] or [i for i in range(1, amount) if holding[i] < limit]
        pool, left = sum([loads[i] for i in candidates]), spare
        for i in candidates:
            more = min(limit - holding[i], max(1, left * loads[i] // pool), spare)
            holding[i] = holding[i] + more
            spare = spare - more
    return np.array(holding)


def gaussian(rng, extent, deviation, limit, cuts=(), held_as=jnp.bfloat16):
    loudness = level_of(rng, extent, cuts, -0.22, 0.18) if cuts else 1.0
    entries = jax.random.normal(rng, extent, jnp.float32) * deviation * loudness
    return jnp.minimum(jnp.maximum(entries, -limit), limit).astype(held_as)


def setup_inputs(seed: int = 0) -> dict:
    arg_keys = jax.random.split(jax.random.key(seed), 17)
    pool_in = draw_pool_in(jax.random.fold_in(arg_keys[16], 71), 0)
    doc_ids = jnp.searchsorted(jnp.cumsum(uneven(arg_keys[1], DOCS, TOKENS, DOC_MOST, 1)), jnp.arange(TOKENS), side="right").astype(jnp.int32)
    pool_map = gaussian(arg_keys[2], (GROUPS, GROUP_W, GROUP_W), GROUP_W ** -0.5, 0.75)
    pool_scale = jnp.clip(1.0 + 0.18 * jax.random.normal(arg_keys[3], (MIX_W,), jnp.float32), 0.1, 1.9)
    w_out = gaussian(arg_keys[4], (MIX_W, D), MIX_W ** -0.5, 0.25, ((1, 4),))
    gate_logit = gaussian(arg_keys[5], (TOKENS, D), 1.5, 8.0, ((0, 8), (1, 4)))
    residual = gaussian(arg_keys[6], (TOKENS, D), 0.6, 4.0, ((0, 8), (1, 4)))
    first_gain = jnp.clip(1.0 + 0.18 * jax.random.normal(arg_keys[7], (D,), jnp.float32), 0.1, 1.9)
    first_bias = gaussian(arg_keys[8], (D,), 0.3, 1.5, ((0, 4),), jnp.float32)
    routes_keys = jax.random.split(jax.random.fold_in(arg_keys[9], 1), TOKENS // TOK_DEV)
    routes_turns = jax.random.permutation(jax.random.fold_in(arg_keys[9], 3), TOKENS // TOK_DEV)
    routes = jax.vmap(lambda own, number: routed_block(jax.random.fold_in(arg_keys[9], 2), own, number, TOK_DEV, EXPERTS, TOPK, CAP, 1))(routes_keys, routes_turns).reshape((TOKENS, TOPK))
    route_weight = jnp.clip(0.25 + 0.75 * jax.random.uniform(arg_keys[10], (TOKENS, TOPK), jnp.float32) ** level_of(arg_keys[10], (TOKENS, TOPK), ((0, 8),), -0.2, 0.2), 0.25, 1.0)
    w_gate = gaussian(arg_keys[11], (EXPERTS, D, DE), D ** -0.5, 0.125, ((0, 8), (2, 4)))
    w_up = gaussian(arg_keys[12], (EXPERTS, D, DE), D ** -0.5, 0.125, ((0, 8), (2, 4)))
    w_down = gaussian(arg_keys[13], (EXPERTS, DE, D), (DE // 4) ** -0.5, 0.375, ((0, 8), (2, 4)))
    second_gain = jnp.clip(1.0 + 0.18 * jax.random.normal(arg_keys[14], (D,), jnp.float32), 0.1, 1.9)
    second_bias = gaussian(arg_keys[15], (D,), 0.3, 1.5, ((0, 4),), jnp.float32)
    return dict(pool_in=pool_in, doc_ids=doc_ids, pool_map=pool_map, pool_scale=pool_scale, w_out=w_out, gate_logit=gate_logit, residual=residual, first_gain=first_gain, first_bias=first_bias, routes=routes, route_weight=route_weight, w_gate=w_gate, w_up=w_up, w_down=w_down, second_gain=second_gain, second_bias=second_bias)


EPS = 1e-05
ALPHA = 8.0 ** 0.25

def layer_norm(row_data, gain_vec, bias_vec):
    row_mean = lax.optimization_barrier(jnp.mean(row_data, axis=1, keepdims=True))
    row_var = lax.optimization_barrier(jnp.mean(row_data * row_data, axis=1, keepdims=True)) - row_mean * row_mean
    return (row_data - row_mean) * lax.rsqrt(row_var + EPS) * gain_vec + bias_vec

def pool_scales(pool_in, doc_ids):
    values = pool_in.astype(jnp.float32)
    length = values.shape[1]
    opening = jnp.concatenate([jnp.ones((1,), bool), doc_ids[1:] != doc_ids[:-1]])
    places = jnp.arange(length, dtype=jnp.int32)
    doc_start = lax.cummax(jnp.where(opening, places, 0), axis=0)
    prefix = jnp.concatenate([jnp.zeros((MIX_W, 1), jnp.float32), jnp.cumsum(values, axis=1)], axis=1)
    upper_at = places + 1
    group_id = jnp.arange(MIX_W, dtype=jnp.int32) // GROUP_W
    doc_mask = (group_id % 2 == 1)[:, None]
    window = jnp.left_shift(2, group_id // 2 % 4)[:, None]
    lower_at = jnp.where(doc_mask, doc_start[None, :], jnp.maximum(upper_at[None, :] - window, doc_start[None, :]))
    lower_at = lower_at.astype(jnp.int32)
    window_sum = prefix[:, 1:] - jnp.take_along_axis(prefix, lower_at, axis=1)
    counted = (upper_at[None, :] - lower_at).astype(jnp.float32)
    return (window_sum / counted - values).astype(jnp.bfloat16)

def reference(pool_in, doc_ids, pool_map, pool_scale, w_out, gate_logit, residual, first_gain, first_bias, routes, route_weight, w_gate, w_up, w_down, second_gain, second_bias):
    pooled = pool_scales(pool_in, doc_ids)
    grouped = jnp.einsum('gct,gcd->tgd', pooled.reshape(GROUPS, GROUP_W, TOKENS).astype(jnp.float32), pool_map.astype(jnp.float32))
    mapped = (grouped.reshape(TOKENS, MIX_W) * pool_scale).astype(jnp.bfloat16)
    mixer_out = jnp.dot(mapped, w_out, preferred_element_type=jnp.float32) * jax.nn.sigmoid(gate_logit.astype(jnp.float32))
    normed = layer_norm(ALPHA * residual.astype(jnp.float32) + mixer_out, first_gain, first_bias).astype(jnp.bfloat16)
    flat_routes = routes.reshape(-1).astype(jnp.int32)
    one_hot = (flat_routes[:, None] == jnp.arange(EXPERTS, dtype=jnp.int32)[None, :]).astype(jnp.int32)
    slot_rank = lax.optimization_barrier(jnp.sum((jnp.cumsum(one_hot, axis=0, dtype=jnp.int32) - 1) * one_hot, axis=1)).astype(jnp.int32)
    rows_most = N_SP * CAP
    token_of = jnp.arange(TOKENS * TOPK, dtype=jnp.int32) // TOPK
    flat_weight = route_weight.reshape(-1)

    def one_expert(running, expert):
        slot_ids = jnp.where(flat_routes == expert, slot_rank, rows_most).astype(jnp.int32)
        picked = jnp.zeros((rows_most,), jnp.int32).at[slot_ids].set(token_of, mode='drop')
        slot_weight = jnp.zeros((rows_most,), jnp.float32).at[slot_ids].set(flat_weight, mode='drop')
        inputs = normed[picked]
        gate_part = jnp.dot(inputs, w_gate[expert], preferred_element_type=jnp.float32)
        up_part = jnp.dot(inputs, w_up[expert], preferred_element_type=jnp.float32)
        hidden = (jax.nn.silu(gate_part) * up_part).astype(jnp.bfloat16)
        result = jnp.dot(hidden, w_down[expert], preferred_element_type=jnp.float32).astype(jnp.bfloat16)
        return (running.at[picked].add(slot_weight[:, None] * result.astype(jnp.float32)), None)
    moe_sum, _ = lax.scan(one_expert, jnp.zeros((TOKENS, D), jnp.float32), jnp.arange(EXPERTS, dtype=jnp.int32))
    return layer_norm(ALPHA * normed.astype(jnp.float32) + moe_sum, second_gain, second_bias).astype(jnp.bfloat16)
```

```python
import jax
import jax.numpy as jnp
from jax import lax
from jax.sharding import PartitionSpec as P


GROUP_W = 64
EPS = 1e-05
ALPHA = 8.0**0.25
HALO = 16
F32 = jnp.float32
BF16 = jnp.bfloat16


def swap_with(part, axis, bits):
    size = lax.axis_size(axis)
    return lax.ppermute(part, axis, [(i, i ^ bits) for i in range(size)])


def in_order(relative, index):
    stacked = jnp.stack(relative)
    return [
        lax.dynamic_index_in_dim(stacked, index ^ p, 0, keepdims=False)
        for p in range(len(relative))
    ]


def exchange_all(part, axis):
    return [part] + [swap_with(part, axis, k) for k in range(1, lax.axis_size(axis))]


def line_gather(part, axis):
    size = lax.axis_size(axis)
    mine = [part] + [swap_with(part, axis, 2 * k) for k in range(1, size // 2)]
    return mine + [swap_with(m, axis, 1) for m in mine]


def norm_rows(rows, features):
    mean = sum(jnp.sum(r, axis=1, keepdims=True) for r in rows) / features
    square = sum(jnp.sum(r * r, axis=1, keepdims=True) for r in rows) / features
    scale = lax.rsqrt(square - mean * mean + EPS)
    return [(r - mean) * scale for r in rows]


def weight_parts(w_gate, w_up, w_down, tp):
    if tp != 4:
        return tuple(exchange_all(w, "tp") for w in (w_gate, w_up, w_down))
    half = w_gate.shape[0] // 2
    gate1_top = swap_with(w_gate[:half], "tp", 1)
    up2_top = swap_with(w_up[:half], "tp", 2)
    gate1_low = swap_with(w_gate[half:], "tp", 1)
    up2_low = swap_with(w_up[half:], "tp", 2)
    up1 = swap_with(w_up, "tp", 1)
    gate2 = swap_with(w_gate, "tp", 2)
    up3_top = swap_with(up2_top, "tp", 1)
    up3_low = swap_with(up2_low, "tp", 1)
    gate3_top = swap_with(gate1_top, "tp", 2)
    gate3_low = swap_with(gate1_low, "tp", 2)
    down1 = swap_with(w_down, "tp", 1)
    down2 = swap_with(w_down, "tp", 2)
    dhalf = w_down.shape[0] // 2
    down3_low = swap_with(down2[dhalf:], "tp", 1)
    down3_top = swap_with(down1[:dhalf], "tp", 2)
    gate = [
        w_gate,
        jnp.concatenate([gate1_top, gate1_low]),
        gate2,
        jnp.concatenate([gate3_top, gate3_low]),
    ]
    up = [
        w_up,
        up1,
        jnp.concatenate([up2_top, up2_low]),
        jnp.concatenate([up3_top, up3_low]),
    ]
    down = [w_down, down1, down2, jnp.concatenate([down3_top, down3_low])]
    return gate, up, down


def body(
    pool_in,
    doc_ids,
    pool_map,
    pool_scale,
    w_out,
    gate_logit,
    residual,
    first_gain,
    first_bias,
    routes,
    route_weight,
    w_gate,
    w_up,
    w_down,
    second_gain,
    second_bias,
):
    sp, tp = lax.axis_size("sp"), lax.axis_size("tp")
    i, j = lax.axis_index("sp"), lax.axis_index("tp")
    channels, positions = pool_in.shape
    width = residual.shape[1]
    features = width * tp
    quarter = positions // tp
    pairs = routes.shape[1]

    docs = doc_ids.astype(F32)
    values = pool_in.astype(F32)
    ending = docs == docs[positions - 1]
    tail_sum = jnp.sum(jnp.where(ending[None, :], values, 0.0), axis=1)
    tail_count = jnp.sum(ending.astype(F32))
    halo = values[:, positions - HALO :]
    my_routes = lax.dynamic_slice_in_dim(routes, j * quarter, quarter, 0)
    my_weights = lax.dynamic_slice_in_dim(route_weight, j * quarter, quarter, 0)
    lead = jnp.concatenate([docs[positions - HALO :], tail_count[None]])
    flat = jnp.concatenate(
        [
            tail_sum,
            halo.reshape(-1),
            lead,
            my_routes.astype(F32).T.reshape(-1),
            my_weights.T.reshape(-1),
        ]
    )
    used = flat.shape[0]
    rows = -(-used // 128)
    flat = jnp.pad(flat, (0, rows * 128 - used)).reshape(rows, 128)
    pair = jnp.stack([flat, swap_with(flat, "sp", 1)])
    by_z = [pair] + [swap_with(pair, "sp", 2 * k) for k in range(1, sp // 2)]
    rel = [by_z[k // 2][k % 2].reshape(-1)[:used] for k in range(sp)]

    c1 = channels
    c2 = c1 + channels * HALO
    c3 = c2 + HALO + 1
    c4 = c3 + pairs * quarter
    carried_sum = jnp.zeros((channels,), F32)
    carried_count = jnp.zeros((), F32)
    prev = jnp.zeros((c3,), F32)
    for k in range(1, sp):
        source = i ^ k
        same = (source < i) & (rel[k][c2 + HALO - 1] == docs[0])
        carried_sum = carried_sum + jnp.where(same, rel[k][:c1], 0.0)
        carried_count = carried_count + jnp.where(same, rel[k][c2 + HALO], 0.0)
        prev = prev + jnp.where(source == i - 1, rel[k][:c3], 0.0)
    halo_in = prev[c1:c2].reshape(channels, HALO).astype(BF16)
    halo_docs = jnp.where(i == 0, -1.0, prev[c2 : c2 + HALO])

    t_at = jnp.arange(positions, dtype=jnp.int32)
    s_at = t_at[:, None]
    same_doc = (docs[:, None] == docs[None, :]) & (s_at <= t_at[None, :])
    local_count = jnp.sum(same_doc.astype(F32), axis=0)
    in_first = docs == docs[0]
    doc_count = local_count + jnp.where(in_first, carried_count, 0.0)
    unit = min(GROUP_W, channels)
    halo_at = jnp.arange(HALO, dtype=jnp.int32) - HALO
    halo_same = halo_docs[:, None] == docs[None, :]
    pooled_units = []
    for u in range(channels // unit):
        group = (j * channels + u * unit) // GROUP_W
        whole_doc = group % 2 == 1
        window = jnp.left_shift(2, group // 2 % 4)
        mask = same_doc & (whole_doc | (s_at > t_at[None, :] - window))
        here = pool_in[u * unit : (u + 1) * unit]
        total = jnp.dot(here, mask.astype(BF16), preferred_element_type=F32)
        halo_mask = halo_same & (halo_at[:, None] > t_at[None, :] - window) & ~whole_doc
        total = total + jnp.dot(
            halo_in[u * unit : (u + 1) * unit],
            halo_mask.astype(BF16),
            preferred_element_type=F32,
        )
        carry_here = carried_sum[u * unit : (u + 1) * unit]
        total = total + jnp.where(
            whole_doc & in_first[None, :], carry_here[:, None], 0.0
        )
        count = jnp.where(
            whole_doc, doc_count, jnp.minimum(doc_count, window.astype(F32))
        )
        pooled_units.append(total / count[None, :] - here.astype(F32))
    pooled = jnp.concatenate(pooled_units).astype(BF16)

    pooled_rel = exchange_all(pooled, "tp")
    gathered = jnp.concatenate(in_order(pooled_rel, j))
    group_count = gathered.shape[0] // GROUP_W
    grouped = jnp.einsum(
        "gct,gcd->tgd",
        gathered.reshape(group_count, GROUP_W, positions),
        pool_map,
        preferred_element_type=F32,
    )
    mapped = (grouped.reshape(positions, group_count * GROUP_W) * pool_scale).astype(BF16)
    mixer_out = jnp.dot(mapped, w_out, preferred_element_type=F32) * jax.nn.sigmoid(
        gate_logit.astype(F32)
    )
    mixed = ALPHA * residual.astype(F32) + mixer_out

    quarters = [
        lax.dynamic_slice_in_dim(mixed, (j ^ k) * quarter, quarter, 0) for k in range(tp)
    ]
    mixed_rel = [quarters[0]] + [swap_with(quarters[k], "tp", k) for k in range(1, tp)]
    gains = exchange_all(
        jnp.stack([first_gain, first_bias, second_gain, second_bias]), "tp"
    )
    normed_rel = [
        (r * gains[k][0] + gains[k][1]).astype(BF16)
        for k, r in enumerate(norm_rows(mixed_rel, features))
    ]
    tokens = jnp.concatenate(in_order(normed_rel, j), axis=1)

    gate_w, up_w, down_w = weight_parts(w_gate[0], w_up[0], w_down[0], tp)

    everyone = line_gather(tokens, "sp")
    inputs = jnp.concatenate(everyone)
    order = [2 * k for k in range(sp // 2)] + [2 * k + 1 for k in range(sp // 2)]
    mine = i.astype(F32)
    gate_cols = []
    for k in order:
        chosen = rel[k][c3:c4].reshape(pairs, quarter) == mine
        gate_cols.append(
            jnp.sum(jnp.where(chosen, rel[k][c4:].reshape(pairs, quarter), 0.0), axis=0)
        )
    share = jnp.concatenate(gate_cols)[:, None]

    hidden_rel = []
    for k in range(tp):
        gate_part = jnp.dot(inputs, gate_w[k], preferred_element_type=F32)
        up_part = jnp.dot(inputs, up_w[k], preferred_element_type=F32)
        hidden_rel.append((jax.nn.silu(gate_part) * up_part).astype(BF16))
    hidden = jnp.concatenate(in_order(hidden_rel, j), axis=1)

    final_rel = []
    half_rows = (sp // 2) * quarter
    for k in range(tp):
        result = jnp.dot(hidden, down_w[k], preferred_element_type=F32)
        partial = (result * share).astype(BF16)
        other = swap_with(partial[half_rows:], "sp", 1)
        joined = partial[:half_rows].astype(F32) + other.astype(F32)
        moe = joined[:quarter]
        sent = joined.astype(BF16)
        for d in range(1, sp // 2):
            got = swap_with(sent[d * quarter : (d + 1) * quarter], "sp", 2 * d)
            moe = moe + got.astype(F32)
        final_rel.append(ALPHA * normed_rel[k].astype(F32) + moe)
    out_rel = [
        (r * gains[k][2] + gains[k][3]).astype(BF16)
        for k, r in enumerate(norm_rows(final_rel, features))
    ]
    home_rel = [out_rel[0]] + [swap_with(out_rel[k], "tp", k) for k in range(1, tp)]
    return jnp.concatenate(in_order(home_rel, j))


def solution(mesh):
    return jax.shard_map(
        body,
        mesh=mesh,
        in_specs=(
            P("tp", "sp"),
            P("sp"),
            P(),
            P(),
            P(None, "tp"),
            P("sp", "tp"),
            P("sp", "tp"),
            P("tp"),
            P("tp"),
            P("sp", None),
            P("sp", None),
            P("sp", None, "tp"),
            P("sp", None, "tp"),
            P("sp", None, "tp"),
            P("tp"),
            P("tp"),
        ),
        out_specs=P("sp", "tp"),
        check_vma=False,
    )
```

```python
import jax
import jax.numpy as jnp
from jax import lax
from jax.experimental import pallas as pl
from jax.experimental.pallas import tpu as pltpu
from jax.sharding import PartitionSpec as P


GROUP_W = 64
EPS = 1e-05
ALPHA = 8.0**0.25
HALO = 16
F32 = jnp.float32
BF16 = jnp.bfloat16


def swap_with(part, axis, bits):
    size = lax.axis_size(axis)
    return lax.ppermute(part, axis, [(i, i ^ bits) for i in range(size)])


def in_order(relative, index):
    stacked = jnp.stack(relative)
    return [
        lax.dynamic_index_in_dim(stacked, index ^ p, 0, keepdims=False)
        for p in range(len(relative))
    ]


def exchange_all(part, axis):
    return [part] + [swap_with(part, axis, k) for k in range(1, lax.axis_size(axis))]


def line_gather(part, axis):
    size = lax.axis_size(axis)
    mine = [part] + [swap_with(part, axis, 2 * k) for k in range(1, size // 2)]
    return mine + [swap_with(m, axis, 1) for m in mine]


TABLE = HALO + 8


def table_kernel(x_ref, docs_ref, table_ref, start_ref):
    channels, positions = x_ref.shape
    docs = jnp.broadcast_to(docs_ref[...], (8, positions))
    lane = lax.broadcasted_iota(jnp.int32, (8, positions), 1)
    opens = (docs != pltpu.roll(docs, 1, 1)) & (lane > 0)
    start = jnp.where(opens, lane, 0)
    step = 1
    while step < positions:
        moved = pltpu.roll(start, step, 1)
        start = jnp.maximum(start, jnp.where(lane >= step, moved, 0))
        step *= 2
    start_ref[...] = start
    last_start = start[:1, positions - 1 :]
    last_doc = docs[:1, positions - 1 :]
    row = lax.broadcasted_iota(jnp.int32, (TABLE, positions), 0)
    col = lax.broadcasted_iota(jnp.int32, (TABLE, positions), 1)
    pick = ((row < HALO) & (col == positions - HALO + row)) | (
        (row == HALO) & (col >= last_start)
    )
    got = lax.dot_general(
        pick.astype(BF16), x_ref[...], (((1,), (1,)), ((), ())), preferred_element_type=F32
    )
    row = lax.broadcasted_iota(jnp.int32, (TABLE, channels), 0)
    got = jnp.where(row == HALO + 1, last_doc.astype(F32), got)
    table_ref[...] = jnp.where(row == HALO + 2, (positions - last_start).astype(F32), got)


def units_of(channels, j):
    unit = min(GROUP_W, channels)
    for u in range(channels // unit):
        group = (j * channels + u * unit) // GROUP_W
        yield slice(u * unit, (u + 1) * unit), group % 2 == 1, lax.shift_left(2, group // 2 % 4)


def local_kernel(place_ref, x_ref, start_ref, sum_ref):
    channels, positions = x_ref.shape
    s_at = lax.broadcasted_iota(jnp.int32, (positions, positions), 0)
    t_at = lax.broadcasted_iota(jnp.int32, (positions, positions), 1)
    for rows, whole_doc, window in units_of(channels, place_ref[1]):
        reach = jnp.where(whole_doc, positions, window)
        lower = jnp.maximum(start_ref[:1, :], t_at[:1, :] + 1 - reach)
        mask = (s_at >= lower) & (s_at <= t_at)
        sum_ref[rows, :] = jnp.dot(
            x_ref[rows, :], mask.astype(BF16), preferred_element_type=F32
        )


def pooled_kernel(place_ref, x_ref, docs_ref, start_ref, sum_ref, *rest):
    *table_refs, out_ref = rest
    channels, positions = x_ref.shape
    i, j = place_ref[0], place_ref[1]
    first_doc = docs_ref[:1, :1].astype(F32)
    before = jnp.zeros((TABLE, channels), F32)
    carried = jnp.zeros((TABLE, channels), F32)
    for k in range(1, 2 * len(table_refs)):
        table = table_refs[k // 2][k % 2]
        earlier = jnp.where((i ^ k) < i, 1.0, 0.0)
        previous = jnp.where((i ^ k) == i - 1, 1.0, 0.0)
        same = jnp.where(table[HALO + 1 : HALO + 2, :1] == first_doc, earlier, 0.0)
        carried = carried + same * table
        before = before + previous * table
    count = carried[HALO + 2 : HALO + 3, :1]
    t_at = lax.broadcasted_iota(jnp.int32, (1, positions), 1)
    start = start_ref[:1, :]
    in_first = jnp.where(start == 0, 1.0, 0.0)
    doc_count = (t_at + 1 - start).astype(F32) + in_first * count
    row = lax.broadcasted_iota(jnp.int32, (TABLE, channels), 0)
    carry_row = jnp.where(row == HALO, carried, 0.0)
    over_first = jnp.broadcast_to(in_first, (TABLE, positions))
    carry = lax.dot_general(
        carry_row,
        over_first,
        (((0,), (0,)), ((), ())),
        precision=lax.Precision.HIGHEST,
        preferred_element_type=F32,
    )
    h_at = lax.broadcasted_iota(jnp.int32, (TABLE, positions), 0) - HALO
    reached = jnp.where(h_at.astype(F32) >= -count, over_first, 0.0)
    reached = jnp.where(h_at < 0, reached, 0.0)
    for rows, whole_doc, window in units_of(channels, j):
        halo_mask = jnp.where(h_at >= t_at + 1 - window, reached, 0.0)
        halo = lax.dot_general(
            before.astype(BF16),
            halo_mask.astype(BF16),
            (((0,), (0,)), ((), ())),
            preferred_element_type=F32,
        )
        whole = jnp.where(whole_doc, 1.0, 0.0)
        total = sum_ref[rows, :] + whole * carry[rows] + (1.0 - whole) * halo[rows]
        most = jnp.where(whole_doc, float(1 << 30), window.astype(F32))
        total = total / jnp.minimum(doc_count, most)
        out_ref[rows, :] = (total - x_ref[rows, :].astype(F32)).astype(BF16)


def in_vmem(count):
    return [pl.BlockSpec(memory_space=pltpu.VMEM)] * count


def pooled_channels(pool_in, doc_ids, place):
    channels, positions = pool_in.shape
    docs = doc_ids.reshape(1, positions)
    scalars = pl.BlockSpec(memory_space=pltpu.SMEM)
    table, start = pl.pallas_call(
        table_kernel,
        out_shape=(
            jax.ShapeDtypeStruct((TABLE, channels), F32),
            jax.ShapeDtypeStruct((8, positions), jnp.int32),
        ),
        in_specs=in_vmem(2),
        out_specs=tuple(in_vmem(2)),
        name="table",
    )(pool_in, docs)
    pair = jnp.stack([table, swap_with(table, "sp", 1)])
    sums = pl.pallas_call(
        local_kernel,
        out_shape=jax.ShapeDtypeStruct((channels, positions), F32),
        in_specs=[scalars] + in_vmem(2),
        out_specs=in_vmem(1)[0],
        name="local",
    )(place, pool_in, start)
    tables = [pair] + [
        swap_with(pair, "sp", 2 * k) for k in range(1, lax.axis_size("sp") // 2)
    ]
    return pl.pallas_call(
        pooled_kernel,
        out_shape=jax.ShapeDtypeStruct((channels, positions), BF16),
        in_specs=[scalars] + in_vmem(4 + len(tables)),
        out_specs=in_vmem(1)[0],
        name="pooled",
    )(place, pool_in, docs, start, sums, *tables)


def norm_rows(rows, features):
    mean = sum(jnp.sum(r, axis=1, keepdims=True) for r in rows) / features
    square = sum(jnp.sum(r * r, axis=1, keepdims=True) for r in rows) / features
    scale = lax.rsqrt(square - mean * mean + EPS)
    return [(r - mean) * scale for r in rows]


def weight_parts(w_gate, w_up, w_down, tp):
    if tp != 4:
        return tuple(exchange_all(w, "tp") for w in (w_gate, w_up, w_down))
    half = w_gate.shape[0] // 2
    gate1_top = swap_with(w_gate[:half], "tp", 1)
    up2_top = swap_with(w_up[:half], "tp", 2)
    gate1_low = swap_with(w_gate[half:], "tp", 1)
    up2_low = swap_with(w_up[half:], "tp", 2)
    up1 = swap_with(w_up, "tp", 1)
    gate2 = swap_with(w_gate, "tp", 2)
    up3_top = swap_with(up2_top, "tp", 1)
    up3_low = swap_with(up2_low, "tp", 1)
    gate3_top = swap_with(gate1_top, "tp", 2)
    gate3_low = swap_with(gate1_low, "tp", 2)
    down1 = swap_with(w_down, "tp", 1)
    down2 = swap_with(w_down, "tp", 2)
    dhalf = w_down.shape[0] // 2
    down3_low = swap_with(down2[dhalf:], "tp", 1)
    down3_top = swap_with(down1[:dhalf], "tp", 2)
    gate = [
        w_gate,
        jnp.concatenate([gate1_top, gate1_low]),
        gate2,
        jnp.concatenate([gate3_top, gate3_low]),
    ]
    up = [
        w_up,
        up1,
        jnp.concatenate([up2_top, up2_low]),
        jnp.concatenate([up3_top, up3_low]),
    ]
    down = [w_down, down1, down2, jnp.concatenate([down3_top, down3_low])]
    return gate, up, down


def body(
    pool_in,
    doc_ids,
    pool_map,
    pool_scale,
    w_out,
    gate_logit,
    residual,
    first_gain,
    first_bias,
    routes,
    route_weight,
    w_gate,
    w_up,
    w_down,
    second_gain,
    second_bias,
):
    sp, tp = lax.axis_size("sp"), lax.axis_size("tp")
    i, j = lax.axis_index("sp"), lax.axis_index("tp")
    _, positions = pool_in.shape
    width = residual.shape[1]
    features = width * tp
    quarter = positions // tp

    pooled = pooled_channels(pool_in, doc_ids, jnp.stack([i, j]))
    pooled_rel = exchange_all(pooled, "tp")
    gathered = jnp.concatenate(in_order(pooled_rel, j))
    group_count = gathered.shape[0] // GROUP_W
    grouped = jnp.einsum(
        "gct,gcd->tgd",
        gathered.reshape(group_count, GROUP_W, positions),
        pool_map,
        preferred_element_type=F32,
    )
    mapped = (grouped.reshape(positions, group_count * GROUP_W) * pool_scale).astype(BF16)
    mixer_out = jnp.dot(mapped, w_out, preferred_element_type=F32) * jax.nn.sigmoid(
        gate_logit.astype(F32)
    )
    mixed = ALPHA * residual.astype(F32) + mixer_out

    quarters = [
        lax.dynamic_slice_in_dim(mixed, (j ^ k) * quarter, quarter, 0) for k in range(tp)
    ]
    scales = jnp.pad(
        jnp.stack([first_gain, first_bias, second_gain, second_bias]), ((0, 4), (0, 0))
    )
    both = [jnp.concatenate([q, scales]) for q in quarters]
    both = [both[0]] + [swap_with(both[k], "tp", k) for k in range(1, tp)]
    mixed_rel = [b[:quarter] for b in both]
    gains = [b[quarter:] for b in both]
    normed_rel = [
        (r * gains[k][0] + gains[k][1]).astype(BF16)
        for k, r in enumerate(norm_rows(mixed_rel, features))
    ]
    tokens = jnp.concatenate(in_order(normed_rel, j), axis=1)

    gate_w, up_w, down_w = weight_parts(w_gate[0], w_up[0], w_down[0], tp)

    everyone = line_gather(tokens, "sp")
    inputs = jnp.concatenate(everyone)
    my_routes = lax.dynamic_slice_in_dim(routes, j * quarter, quarter, 0)
    my_weights = lax.dynamic_slice_in_dim(route_weight, j * quarter, quarter, 0)
    chosen = jnp.stack([my_routes.astype(F32).T, my_weights.T])
    chosen = jnp.concatenate([c[None] for c in line_gather(chosen, "sp")])
    chosen = jnp.where(chosen[:, 0] == i.astype(F32), chosen[:, 1], 0.0)
    share = jnp.sum(chosen, axis=1).reshape(-1, 1)

    hidden_rel = []
    for k in range(tp):
        gate_part = jnp.dot(inputs, gate_w[k], preferred_element_type=F32)
        up_part = jnp.dot(inputs, up_w[k], preferred_element_type=F32)
        hidden_rel.append((jax.nn.silu(gate_part) * up_part).astype(BF16))
    hidden = jnp.concatenate(in_order(hidden_rel, j), axis=1)

    final_rel = []
    half_rows = (sp // 2) * quarter
    for k in range(tp):
        result = jnp.dot(hidden, down_w[k], preferred_element_type=F32)
        partial = (result * share).astype(BF16)
        other = swap_with(partial[half_rows:], "sp", 1)
        joined = partial[:half_rows].astype(F32) + other.astype(F32)
        moe = joined[:quarter]
        sent = joined.astype(BF16)
        for d in range(1, sp // 2):
            got = swap_with(sent[d * quarter : (d + 1) * quarter], "sp", 2 * d)
            moe = moe + got.astype(F32)
        final_rel.append(ALPHA * normed_rel[k].astype(F32) + moe)
    out_rel = [
        (r * gains[k][2] + gains[k][3]).astype(BF16)
        for k, r in enumerate(norm_rows(final_rel, features))
    ]
    home_rel = [out_rel[0]] + [swap_with(out_rel[k], "tp", k) for k in range(1, tp)]
    return jnp.concatenate(in_order(home_rel, j))


def solution(mesh):
    return jax.shard_map(
        body,
        mesh=mesh,
        in_specs=(
            P("tp", "sp"),
            P("sp"),
            P(),
            P(),
            P(None, "tp"),
            P("sp", "tp"),
            P("sp", "tp"),
            P("tp"),
            P("tp"),
            P("sp", None),
            P("sp", None),
            P("sp", None, "tp"),
            P("sp", None, "tp"),
            P("sp", None, "tp"),
            P("tp"),
            P("tp"),
        ),
        out_specs=P("sp", "tp"),
        check_vma=False,
    )
```

```python
import functools

import jax
import jax.numpy as jnp
from jax import lax
from jax.experimental import pallas as pl
from jax.experimental.pallas import tpu as pltpu
from jax.sharding import PartitionSpec as P


GROUP_W = 64
EPS = 1e-05
ALPHA = 8.0**0.25
HALO = 16
F32 = jnp.float32
BF16 = jnp.bfloat16


def swap_with(part, axis, bits):
    size = lax.axis_size(axis)
    return lax.ppermute(part, axis, [(i, i ^ bits) for i in range(size)])


def in_order(relative, index):
    stacked = jnp.stack(relative)
    return [
        lax.dynamic_index_in_dim(stacked, index ^ p, 0, keepdims=False)
        for p in range(len(relative))
    ]


def exchange_all(part, axis):
    return [part] + [swap_with(part, axis, k) for k in range(1, lax.axis_size(axis))]


def line_gather(part, axis):
    size = lax.axis_size(axis)
    mine = [part] + [swap_with(part, axis, 2 * k) for k in range(1, size // 2)]
    return mine + [swap_with(m, axis, 1) for m in mine]


TABLE = HALO + 8


def table_kernel(x_ref, docs_ref, table_ref, start_ref):
    channels, positions = x_ref.shape
    docs = jnp.broadcast_to(docs_ref[...], (8, positions))
    lane = lax.broadcasted_iota(jnp.int32, (8, positions), 1)
    opens = (docs != pltpu.roll(docs, 1, 1)) & (lane > 0)
    start = jnp.where(opens, lane, 0)
    step = 1
    while step < positions:
        moved = pltpu.roll(start, step, 1)
        start = jnp.maximum(start, jnp.where(lane >= step, moved, 0))
        step *= 2
    start_ref[...] = start
    last_start = start[:1, positions - 1 :]
    last_doc = docs[:1, positions - 1 :]
    row = lax.broadcasted_iota(jnp.int32, (TABLE, positions), 0)
    col = lax.broadcasted_iota(jnp.int32, (TABLE, positions), 1)
    pick = ((row < HALO) & (col == positions - HALO + row)) | (
        (row == HALO) & (col >= last_start)
    )
    got = lax.dot_general(
        pick.astype(BF16), x_ref[...], (((1,), (1,)), ((), ())), preferred_element_type=F32
    )
    row = lax.broadcasted_iota(jnp.int32, (TABLE, channels), 0)
    got = jnp.where(row == HALO + 1, last_doc.astype(F32), got)
    table_ref[...] = jnp.where(row == HALO + 2, (positions - last_start).astype(F32), got)


def units_of(channels, j):
    unit = min(GROUP_W, channels)
    for u in range(channels // unit):
        group = (j * channels + u * unit) // GROUP_W
        yield slice(u * unit, (u + 1) * unit), group % 2 == 1, lax.shift_left(2, group // 2 % 4)


def local_kernel(place_ref, x_ref, start_ref, sum_ref):
    channels, positions = x_ref.shape
    s_at = lax.broadcasted_iota(jnp.int32, (positions, positions), 0)
    t_at = lax.broadcasted_iota(jnp.int32, (positions, positions), 1)
    for rows, whole_doc, window in units_of(channels, place_ref[1]):
        reach = jnp.where(whole_doc, positions, window)
        lower = jnp.maximum(start_ref[:1, :], t_at[:1, :] + 1 - reach)
        mask = (s_at >= lower) & (s_at <= t_at)
        sum_ref[rows, :] = jnp.dot(
            x_ref[rows, :], mask.astype(BF16), preferred_element_type=F32
        )


def pooled_kernel(place_ref, x_ref, docs_ref, start_ref, sum_ref, *rest):
    *table_refs, out_ref = rest
    channels, positions = x_ref.shape
    i, j = place_ref[0], place_ref[1]
    first_doc = docs_ref[:1, :1].astype(F32)
    before = jnp.zeros((TABLE, channels), F32)
    carried = jnp.zeros((TABLE, channels), F32)
    for k in range(1, 2 * len(table_refs)):
        table = table_refs[k // 2][k % 2]
        earlier = jnp.where((i ^ k) < i, 1.0, 0.0)
        previous = jnp.where((i ^ k) == i - 1, 1.0, 0.0)
        same = jnp.where(table[HALO + 1 : HALO + 2, :1] == first_doc, earlier, 0.0)
        carried = carried + same * table
        before = before + previous * table
    count = carried[HALO + 2 : HALO + 3, :1]
    t_at = lax.broadcasted_iota(jnp.int32, (1, positions), 1)
    start = start_ref[:1, :]
    in_first = jnp.where(start == 0, 1.0, 0.0)
    doc_count = (t_at + 1 - start).astype(F32) + in_first * count
    row = lax.broadcasted_iota(jnp.int32, (TABLE, channels), 0)
    carry_row = jnp.where(row == HALO, carried, 0.0)
    over_first = jnp.broadcast_to(in_first, (TABLE, positions))
    carry = lax.dot_general(
        carry_row,
        over_first,
        (((0,), (0,)), ((), ())),
        precision=lax.Precision.HIGHEST,
        preferred_element_type=F32,
    )
    h_at = lax.broadcasted_iota(jnp.int32, (TABLE, positions), 0) - HALO
    reached = jnp.where(h_at.astype(F32) >= -count, over_first, 0.0)
    reached = jnp.where(h_at < 0, reached, 0.0)
    for rows, whole_doc, window in units_of(channels, j):
        halo_mask = jnp.where(h_at >= t_at + 1 - window, reached, 0.0)
        halo = lax.dot_general(
            before.astype(BF16),
            halo_mask.astype(BF16),
            (((0,), (0,)), ((), ())),
            preferred_element_type=F32,
        )
        whole = jnp.where(whole_doc, 1.0, 0.0)
        total = sum_ref[rows, :] + whole * carry[rows] + (1.0 - whole) * halo[rows]
        most = jnp.where(whole_doc, float(1 << 30), window.astype(F32))
        total = total / jnp.minimum(doc_count, most)
        out_ref[rows, :] = (total - x_ref[rows, :].astype(F32)).astype(BF16)


def in_vmem(count):
    return [pl.BlockSpec(memory_space=pltpu.VMEM)] * count


def pooled_channels(pool_in, doc_ids, place):
    channels, positions = pool_in.shape
    docs = doc_ids.reshape(1, positions)
    scalars = pl.BlockSpec(memory_space=pltpu.SMEM)
    table, start = pl.pallas_call(
        table_kernel,
        out_shape=(
            jax.ShapeDtypeStruct((TABLE, channels), F32),
            jax.ShapeDtypeStruct((8, positions), jnp.int32),
        ),
        in_specs=in_vmem(2),
        out_specs=tuple(in_vmem(2)),
        name="table",
    )(pool_in, docs)
    pair = jnp.stack([table, swap_with(table, "sp", 1)])
    sums = pl.pallas_call(
        local_kernel,
        out_shape=jax.ShapeDtypeStruct((channels, positions), F32),
        in_specs=[scalars] + in_vmem(2),
        out_specs=in_vmem(1)[0],
        name="local",
    )(place, pool_in, start)
    tables = [pair] + [
        swap_with(pair, "sp", 2 * k) for k in range(1, lax.axis_size("sp") // 2)
    ]
    return pl.pallas_call(
        pooled_kernel,
        out_shape=jax.ShapeDtypeStruct((channels, positions), BF16),
        in_specs=[scalars] + in_vmem(4 + len(tables)),
        out_specs=in_vmem(1)[0],
        name="pooled",
    )(place, pool_in, docs, start, sums, *tables)


def norm_rows(rows, features):
    mean = sum(jnp.sum(r, axis=1, keepdims=True) for r in rows) / features
    square = sum(jnp.sum(r * r, axis=1, keepdims=True) for r in rows) / features
    scale = lax.rsqrt(square - mean * mean + EPS)
    return [(r - mean) * scale for r in rows]


def gather_rows_kernel(*refs):
    *parts, out_ref = refs
    rows = parts[0].shape[0]
    for p, part in enumerate(parts):
        out_ref[p * rows : (p + 1) * rows, :] = part[...]


def hidden_kernel(count, *refs):
    row_refs, rest = refs[: count[0]], refs[count[0] :]
    gates, ups = rest[: count[1]], rest[count[1] : count[1] + count[2]]
    outs = rest[count[1] + count[2] :]
    if len(outs) == 2:
        gather_rows_kernel(*row_refs, outs[0])
        rows = outs[0]
    else:
        rows = row_refs[0]

    def product(parts):
        total, at = None, 0
        for part in parts:
            depth = part.shape[0]
            piece = jnp.dot(
                rows[:, at : at + depth], part[...], preferred_element_type=F32
            )
            total = piece if total is None else total + piece
            at += depth
        return total

    gated = product(gates)
    outs[-1][...] = (gated * jax.nn.sigmoid(gated) * product(ups)).astype(BF16)


def hidden_units(row_parts, gates, ups):
    count = (len(row_parts), len(gates), len(ups))
    rows = sum(r.shape[0] for r in row_parts)
    shape = jax.ShapeDtypeStruct((rows, gates[0].shape[1]), BF16)
    joined = jax.ShapeDtypeStruct((rows, row_parts[0].shape[1]), BF16)
    outs = (joined, shape) if len(row_parts) > 1 else (shape,)
    got = pl.pallas_call(
        functools.partial(hidden_kernel, count),
        out_shape=outs,
        in_specs=in_vmem(sum(count)),
        out_specs=tuple(in_vmem(len(outs))),
        name="hidden",
    )(*row_parts, *gates, *ups)
    return (got[0], got[-1])


def weight_parts(w_gate, w_up, w_down, tp):
    if tp != 4:
        gate, up, down = (exchange_all(w, "tp") for w in (w_gate, w_up, w_down))
        return [[w] for w in gate], [[w] for w in up], down
    half = w_gate.shape[0] // 2
    gate1_top = swap_with(w_gate[:half], "tp", 1)
    up2_top = swap_with(w_up[:half], "tp", 2)
    gate1_low = swap_with(w_gate[half:], "tp", 1)
    up2_low = swap_with(w_up[half:], "tp", 2)
    up1 = swap_with(w_up, "tp", 1)
    gate2 = swap_with(w_gate, "tp", 2)
    up3_top = swap_with(up2_top, "tp", 1)
    up3_low = swap_with(up2_low, "tp", 1)
    gate3_top = swap_with(gate1_top, "tp", 2)
    gate3_low = swap_with(gate1_low, "tp", 2)
    down1 = swap_with(w_down, "tp", 1)
    down2 = swap_with(w_down, "tp", 2)
    dhalf = w_down.shape[0] // 2
    down3_low = swap_with(down2[dhalf:], "tp", 1)
    down3_top = swap_with(down1[:dhalf], "tp", 2)
    gate = [[w_gate], [gate1_top, gate1_low], [gate2], [gate3_top, gate3_low]]
    up = [[w_up], [up1], [up2_top, up2_low], [up3_top, up3_low]]
    down = [w_down, down1, down2, jnp.concatenate([down3_top, down3_low])]
    return gate, up, down


def body(
    pool_in,
    doc_ids,
    pool_map,
    pool_scale,
    w_out,
    gate_logit,
    residual,
    first_gain,
    first_bias,
    routes,
    route_weight,
    w_gate,
    w_up,
    w_down,
    second_gain,
    second_bias,
):
    sp, tp = lax.axis_size("sp"), lax.axis_size("tp")
    i, j = lax.axis_index("sp"), lax.axis_index("tp")
    _, positions = pool_in.shape
    width = residual.shape[1]
    features = width * tp
    quarter = positions // tp

    pooled = pooled_channels(pool_in, doc_ids, jnp.stack([i, j]))
    pooled_rel = exchange_all(pooled, "tp")
    gathered = jnp.concatenate(in_order(pooled_rel, j))
    group_count = gathered.shape[0] // GROUP_W
    grouped = jnp.einsum(
        "gct,gcd->tgd",
        gathered.reshape(group_count, GROUP_W, positions),
        pool_map,
        preferred_element_type=F32,
    )
    mapped = (grouped.reshape(positions, group_count * GROUP_W) * pool_scale).astype(BF16)
    mixer_out = jnp.dot(mapped, w_out, preferred_element_type=F32) * jax.nn.sigmoid(
        gate_logit.astype(F32)
    )
    mixed = ALPHA * residual.astype(F32) + mixer_out

    quarters = [
        lax.dynamic_slice_in_dim(mixed, (j ^ k) * quarter, quarter, 0) for k in range(tp)
    ]
    scales = jnp.pad(
        jnp.stack([first_gain, first_bias, second_gain, second_bias]), ((0, 4), (0, 0))
    )
    both = [jnp.concatenate([q, scales]) for q in quarters]
    both = [both[0]] + [swap_with(both[k], "tp", k) for k in range(1, tp)]
    mixed_rel = [b[:quarter] for b in both]
    gains = [b[quarter:] for b in both]
    normed_rel = [
        (r * gains[k][0] + gains[k][1]).astype(BF16)
        for k, r in enumerate(norm_rows(mixed_rel, features))
    ]
    tokens = jnp.concatenate(in_order(normed_rel, j), axis=1)

    gate_w, up_w, down_w = weight_parts(w_gate[0], w_up[0], w_down[0], tp)

    everyone = line_gather(tokens, "sp")
    my_routes = lax.dynamic_slice_in_dim(routes, j * quarter, quarter, 0)
    my_weights = lax.dynamic_slice_in_dim(route_weight, j * quarter, quarter, 0)
    chosen = jnp.stack([my_routes.astype(F32).T, my_weights.T])
    chosen = jnp.concatenate([c[None] for c in line_gather(chosen, "sp")])
    chosen = jnp.where(chosen[:, 0] == i.astype(F32), chosen[:, 1], 0.0)
    share = jnp.sum(chosen, axis=1).reshape(-1, 1)

    inputs, first_hidden = hidden_units(everyone, gate_w[0], up_w[0])
    hidden_rel = [first_hidden] + [
        hidden_units([inputs], gate_w[k], up_w[k])[1] for k in range(1, tp)
    ]
    hidden = jnp.concatenate(in_order(hidden_rel, j), axis=1)

    final_rel = []
    half_rows = (sp // 2) * quarter
    for k in range(tp):
        result = jnp.dot(hidden, down_w[k], preferred_element_type=F32)
        partial = (result * share).astype(BF16)
        other = swap_with(partial[half_rows:], "sp", 1)
        joined = partial[:half_rows].astype(F32) + other.astype(F32)
        moe = joined[:quarter]
        sent = joined.astype(BF16)
        for d in range(1, sp // 2):
            got = swap_with(sent[d * quarter : (d + 1) * quarter], "sp", 2 * d)
            moe = moe + got.astype(F32)
        final_rel.append(ALPHA * normed_rel[k].astype(F32) + moe)
    out_rel = [
        (r * gains[k][2] + gains[k][3]).astype(BF16)
        for k, r in enumerate(norm_rows(final_rel, features))
    ]
    home_rel = [out_rel[0]] + [swap_with(out_rel[k], "tp", k) for k in range(1, tp)]
    return jnp.concatenate(in_order(home_rel, j))


def solution(mesh):
    return jax.shard_map(
        body,
        mesh=mesh,
        in_specs=(
            P("tp", "sp"),
            P("sp"),
            P(),
            P(),
            P(None, "tp"),
            P("sp", "tp"),
            P("sp", "tp"),
            P("tp"),
            P("tp"),
            P("sp", None),
            P("sp", None),
            P("sp", None, "tp"),
            P("sp", None, "tp"),
            P("sp", None, "tp"),
            P("tp"),
            P("tp"),
        ),
        out_specs=P("sp", "tp"),
        check_vma=False,
    )
```

```python
import functools

import jax
import jax.numpy as jnp
from jax import lax
from jax.experimental import pallas as pl
from jax.experimental.pallas import tpu as pltpu
from jax.sharding import PartitionSpec as P


GROUP_W = 64
EPS = 1e-05
ALPHA = 8.0**0.25
HALO = 16
F32 = jnp.float32
BF16 = jnp.bfloat16


def swap_with(part, axis, bits):
    size = lax.axis_size(axis)
    return lax.ppermute(part, axis, [(i, i ^ bits) for i in range(size)])


def in_order(relative, index):
    stacked = jnp.stack(relative)
    return [
        lax.dynamic_index_in_dim(stacked, index ^ p, 0, keepdims=False)
        for p in range(len(relative))
    ]


def exchange_all(part, axis):
    return [part] + [swap_with(part, axis, k) for k in range(1, lax.axis_size(axis))]


def line_gather(part, axis):
    size = lax.axis_size(axis)
    mine = [part]
    for k in range(1, size // 2):
        mine.append(swap_with(part, axis, 2 * k))
    return mine + [swap_with(m, axis, 1) for m in mine]


TABLE = HALO + 8


def table_kernel(x_ref, docs_ref, table_ref):
    channels, positions = x_ref.shape
    docs = docs_ref[...].astype(F32).reshape(1, positions)
    last_doc = docs[:, positions - 1 :]
    ending = jnp.where(docs == last_doc, 1.0, 0.0)
    length = jnp.sum(ending, axis=1, keepdims=True)
    row = lax.broadcasted_iota(jnp.int32, (TABLE, positions), 0)
    col = lax.broadcasted_iota(jnp.int32, (TABLE, positions), 1)
    pick = jnp.where(col == positions - HALO + row, 1.0, 0.0)
    pick = jnp.where(row == HALO, jnp.broadcast_to(ending, pick.shape), pick)
    got = lax.dot_general(
        pick.astype(BF16), x_ref[...], (((1,), (1,)), ((), ())), preferred_element_type=F32
    )
    row = lax.broadcasted_iota(jnp.int32, (TABLE, channels), 0)
    got = jnp.where(row == HALO + 1, last_doc, got)
    table_ref[...] = jnp.where(row == HALO + 2, length, got)


def starts_of(docs_ref, positions):
    docs = jnp.broadcast_to(docs_ref[...].reshape(1, positions), (8, positions))
    lane = lax.broadcasted_iota(jnp.int32, (8, positions), 1)
    opens = (docs != pltpu.roll(docs, 1, 1)) & (lane > 0)
    start = jnp.where(opens, lane, 0)
    step = 1
    while step < positions:
        moved = pltpu.roll(start, step, 1)
        start = jnp.maximum(start, jnp.where(lane >= step, moved, 0))
        step *= 2
    return start


def units_of(channels, j):
    unit = min(GROUP_W, channels)
    for u in range(channels // unit):
        group = (j * channels + u * unit) // GROUP_W
        yield slice(u * unit, (u + 1) * unit), group % 2 == 1, lax.shift_left(2, group // 2 % 4)


def local_kernel(place_ref, x_ref, docs_ref, sum_ref, start_ref):
    channels, positions = x_ref.shape
    start_ref[...] = starts_of(docs_ref, positions)
    s_at = lax.broadcasted_iota(jnp.int32, (positions, positions), 0)
    t_at = lax.broadcasted_iota(jnp.int32, (positions, positions), 1)
    for rows, whole_doc, window in units_of(channels, place_ref[1]):
        reach = jnp.where(whole_doc, positions, window)
        lower = jnp.maximum(start_ref[:1, :], t_at[:1, :] + 1 - reach)
        mask = (s_at >= lower) & (s_at <= t_at)
        sum_ref[rows, :] = jnp.dot(
            x_ref[rows, :], mask.astype(BF16), preferred_element_type=F32
        )


def pooled_kernel(place_ref, x_ref, docs_ref, start_ref, sum_ref, *rest):
    *table_refs, out_ref = rest
    channels, positions = x_ref.shape
    i, j = place_ref[0], place_ref[1]
    first_doc = docs_ref[...].astype(F32).reshape(1, positions)[:, :1]
    before = jnp.zeros((TABLE, channels), F32)
    carried = jnp.zeros((TABLE, channels), F32)
    near_ref, *far_refs = table_refs
    for k in range(1, 2 * len(table_refs)):
        table = near_ref[...] if k == 1 else far_refs[k // 2 - 1][k % 2]
        earlier = jnp.where((i ^ k) < i, 1.0, 0.0)
        previous = jnp.where((i ^ k) == i - 1, 1.0, 0.0)
        same = jnp.where(table[HALO + 1 : HALO + 2, :1] == first_doc, earlier, 0.0)
        carried = carried + same * table
        before = before + previous * table
    count = carried[HALO + 2 : HALO + 3, :1]
    t_at = lax.broadcasted_iota(jnp.int32, (1, positions), 1)
    start = start_ref[:1, :]
    in_first = jnp.where(start == 0, 1.0, 0.0)
    doc_count = (t_at + 1 - start).astype(F32) + in_first * count
    row = lax.broadcasted_iota(jnp.int32, (TABLE, channels), 0)
    carry_row = jnp.where(row == HALO, carried, 0.0)
    over_first = jnp.broadcast_to(in_first, (TABLE, positions))
    carry = lax.dot_general(
        carry_row,
        over_first,
        (((0,), (0,)), ((), ())),
        precision=lax.Precision.HIGHEST,
        preferred_element_type=F32,
    )
    h_at = lax.broadcasted_iota(jnp.int32, (TABLE, positions), 0) - HALO
    reached = jnp.where(h_at.astype(F32) >= -count, over_first, 0.0)
    reached = jnp.where(h_at < 0, reached, 0.0)
    for rows, whole_doc, window in units_of(channels, j):
        halo_mask = jnp.where(h_at >= t_at + 1 - window, reached, 0.0)
        halo = lax.dot_general(
            before.astype(BF16),
            halo_mask.astype(BF16),
            (((0,), (0,)), ((), ())),
            preferred_element_type=F32,
        )
        whole = jnp.where(whole_doc, 1.0, 0.0)
        total = sum_ref[rows, :] + whole * carry[rows] + (1.0 - whole) * halo[rows]
        most = jnp.where(whole_doc, float(1 << 30), window.astype(F32))
        total = total / jnp.minimum(doc_count, most)
        out_ref[rows, :] = (total - x_ref[rows, :].astype(F32)).astype(BF16)


def in_vmem(count):
    return [pl.BlockSpec(memory_space=pltpu.VMEM)] * count


def room(mebibytes):
    return pltpu.CompilerParams(vmem_limit_bytes=mebibytes << 20)


def pooled_channels(pool_in, doc_ids, place):
    channels, positions = pool_in.shape
    scalars = pl.BlockSpec(memory_space=pltpu.SMEM)
    table = pl.pallas_call(
        table_kernel,
        out_shape=jax.ShapeDtypeStruct((TABLE, channels), F32),
        in_specs=in_vmem(2),
        out_specs=in_vmem(1)[0],
        compiler_params=room(4),
        name="table",
    )(pool_in, doc_ids)
    near = swap_with(table, "sp", 1)
    pair = jnp.stack([table, near])
    sums, start = pl.pallas_call(
        local_kernel,
        out_shape=(
            jax.ShapeDtypeStruct((channels, positions), F32),
            jax.ShapeDtypeStruct((8, positions), jnp.int32),
        ),
        in_specs=[scalars] + in_vmem(2),
        out_specs=tuple(in_vmem(2)),
        compiler_params=room(8),
        name="local",
    )(place, pool_in, doc_ids)
    far = [swap_with(pair, "sp", 2 * k) for k in range(1, lax.axis_size("sp") // 2)]
    return pl.pallas_call(
        pooled_kernel,
        out_shape=jax.ShapeDtypeStruct((channels, positions), BF16),
        in_specs=[scalars] + in_vmem(5 + len(far)),
        out_specs=in_vmem(1)[0],
        compiler_params=room(8),
        name="pooled",
    )(place, pool_in, doc_ids, start, sums, near, *far)


def norm_rows(rows, features):
    mean = sum(jnp.sum(r, axis=1, keepdims=True) for r in rows) / features
    square = sum(jnp.sum(r * r, axis=1, keepdims=True) for r in rows) / features
    scale = lax.rsqrt(square - mean * mean + EPS)
    return [(r - mean) * scale for r in rows]


def gather_rows_kernel(*refs):
    *parts, out_ref = refs
    rows = parts[0].shape[0]
    for p, part in enumerate(parts):
        out_ref[p * rows : (p + 1) * rows, :] = part[...]


def hidden_kernel(count, *refs):
    row_refs, weights, outs = refs[:count], refs[count:-1], refs[-1:]
    if count > 1:
        weights, outs = refs[count:-2], refs[-2:]
        gather_rows_kernel(*row_refs, outs[0])
    rows = outs[0] if count > 1 else row_refs[0]
    if len(weights) == 1:
        both = jnp.dot(rows[...], weights[0][...], preferred_element_type=F32)
        half = both.shape[1] // 2
        gated, up = both[:, :half], both[:, half:]
    else:
        gated, up = (
            jnp.dot(rows[...], w[...], preferred_element_type=F32) for w in weights
        )
    outs[-1][...] = (gated * jax.nn.sigmoid(gated) * up).astype(BF16)


def hidden_units(row_parts, weights):
    count = len(row_parts)
    rows = sum(r.shape[0] for r in row_parts)
    wide = sum(w.shape[1] for w in weights) // 2
    shape = jax.ShapeDtypeStruct((rows, wide), BF16)
    joined = jax.ShapeDtypeStruct((rows, row_parts[0].shape[1]), BF16)
    outs = (joined, shape) if count > 1 else (shape,)
    got = pl.pallas_call(
        functools.partial(hidden_kernel, count),
        out_shape=outs,
        in_specs=in_vmem(count + len(weights)),
        out_specs=tuple(in_vmem(len(outs))),
        compiler_params=room(20),
        name="hidden",
    )(*row_parts, *weights)
    return (got[0], got[-1])


def stage_kernel(*refs):
    parts = len(refs) // 3
    for k in range(parts):
        half = refs[2 * k].shape[1]
        refs[2 * parts + k][:, :half] = refs[2 * k][...]
        refs[2 * parts + k][:, half:] = refs[2 * k + 1][...]


def staged(pairs):
    flat = [w for pair in pairs for w in pair]
    return pl.pallas_call(
        stage_kernel,
        out_shape=tuple(
            jax.ShapeDtypeStruct((g.shape[0], 2 * g.shape[1]), BF16) for g, _ in pairs
        ),
        in_specs=in_vmem(len(flat)),
        out_specs=tuple(in_vmem(len(pairs))),
        compiler_params=room(16),
        name="stage",
    )(*flat)


def down_kernel(parts, place_ref, share_ref, *refs):
    hidden, weights, out_ref = refs[:parts], refs[parts:-1], refs[-1]
    depth, at = hidden[0].shape[1], 0
    for weight in weights:
        total = None
        for k in range(parts):
            rows = pl.ds(pl.multiple_of((place_ref[1] ^ k) * depth, depth), depth)
            piece = jnp.dot(hidden[k][...], weight[rows, :], preferred_element_type=F32)
            total = piece if total is None else total + piece
        wide = weight.shape[1]
        out_ref[:, at : at + wide] = (total * share_ref[...]).astype(BF16)
        at += wide


def weighted_outputs(place, share, hidden, weights):
    wide = sum(w.shape[1] for w in weights)
    return pl.pallas_call(
        functools.partial(down_kernel, len(hidden)),
        out_shape=jax.ShapeDtypeStruct((hidden[0].shape[0], wide), BF16),
        in_specs=[pl.BlockSpec(memory_space=pltpu.SMEM)]
        + in_vmem(1 + len(hidden) + len(weights)),
        out_specs=in_vmem(1)[0],
        compiler_params=room(14),
        name="down",
    )(place, share, *hidden, *weights)


def first_norm_kernel(parts, place_ref, *refs):
    rows, (tokens_ref, normed_ref, scale_ref) = refs[:parts], refs[parts:]
    count, wide = normed_ref.shape[1:]
    total = square = 0.0
    for ref in rows:
        part = ref[:count, :]
        total = total + jnp.sum(part, axis=1, keepdims=True)
        square = square + jnp.sum(part * part, axis=1, keepdims=True)
    mean = total / (parts * wide)
    scale = lax.rsqrt(square / (parts * wide) - mean * mean + EPS)
    for k, ref in enumerate(rows):
        gains = ref[count:, :]
        scale_ref[k] = gains
        part = (ref[:count, :] - mean) * scale * gains[:1] + gains[1:2]
        part = part.astype(BF16)
        normed_ref[k] = part
        at = pl.multiple_of((place_ref[1] ^ k) * wide, wide)
        tokens_ref[:, pl.ds(at, wide)] = part


def first_norm(place, rows, count):
    parts, wide = len(rows), rows[0].shape[1]
    tokens, normed, scales = pl.pallas_call(
        functools.partial(first_norm_kernel, parts),
        out_shape=(
            jax.ShapeDtypeStruct((count, parts * wide), BF16),
            jax.ShapeDtypeStruct((parts, count, wide), BF16),
            jax.ShapeDtypeStruct((parts, rows[0].shape[0] - count, wide), F32),
        ),
        in_specs=[pl.BlockSpec(memory_space=pltpu.SMEM)] + in_vmem(parts),
        out_specs=tuple(in_vmem(3)),
        compiler_params=room(8),
        name="norm",
    )(place, *rows)
    return tokens, [normed[k] for k in range(parts)], [scales[k] for k in range(parts)]


def weight_parts(w_gate, w_up, w_down, tp):
    if tp != 4:
        gate, up, down = (exchange_all(w, "tp") for w in (w_gate, w_up, w_down))
        return [list(pair) for pair in zip(gate, up)], [[w] for w in down]
    gate1 = swap_with(w_gate, "tp", 1)
    up2 = swap_with(w_up, "tp", 2)
    up1 = swap_with(w_up, "tp", 1)
    gate2 = swap_with(w_gate, "tp", 2)
    up3 = swap_with(up2, "tp", 1)
    gate3 = swap_with(gate1, "tp", 2)
    wide = w_down.shape[1] // 2
    left, right = w_down[:, :wide], w_down[:, wide:]
    down1_left = swap_with(left, "tp", 1)
    down2_right = swap_with(right, "tp", 2)
    down1_right = swap_with(right, "tp", 1)
    down2_left = swap_with(left, "tp", 2)
    down3_right = swap_with(down2_right, "tp", 1)
    down3_left = swap_with(down1_left, "tp", 2)
    near = staged([(w_gate, w_up), (gate1, up1), (gate2, up2)])
    first = [[w] for w in near] + [[gate3, up3]]
    down = [
        [w_down],
        [down1_left, down1_right],
        [down2_left, down2_right],
        [down3_left, down3_right],
    ]
    return first, down


def body(
    pool_in,
    doc_ids,
    pool_map,
    pool_scale,
    w_out,
    gate_logit,
    residual,
    first_gain,
    first_bias,
    routes,
    route_weight,
    w_gate,
    w_up,
    w_down,
    second_gain,
    second_bias,
):
    sp, tp = lax.axis_size("sp"), lax.axis_size("tp")
    i, j = lax.axis_index("sp"), lax.axis_index("tp")
    _, positions = pool_in.shape
    width = residual.shape[1]
    features = width * tp
    quarter = positions // tp

    place = jnp.stack([i, j])
    pooled = pooled_channels(pool_in, doc_ids, place)
    pooled_rel = exchange_all(pooled, "tp")
    my_routes = lax.dynamic_slice_in_dim(routes, j * quarter, quarter, 0)
    my_weights = lax.dynamic_slice_in_dim(route_weight, j * quarter, quarter, 0)
    chosen = jnp.stack([my_routes.astype(F32).T, my_weights.T])
    chosen = jnp.stack([chosen, swap_with(chosen, "sp", 1)])
    chosen = [chosen] + [swap_with(chosen, "sp", 2 * k) for k in range(1, sp // 2)]
    chosen = jnp.concatenate([c[core][None] for core in range(2) for c in chosen])
    chosen = jnp.where(chosen[:, 0] == i.astype(F32), chosen[:, 1], 0.0)
    share = jnp.sum(chosen, axis=1).reshape(-1, 1)

    gathered = jnp.concatenate(in_order(pooled_rel, j))
    group_count = gathered.shape[0] // GROUP_W
    grouped = jnp.einsum(
        "gct,gcd->tgd",
        gathered.reshape(group_count, GROUP_W, positions),
        pool_map,
        preferred_element_type=F32,
    )
    mapped = (grouped.reshape(positions, group_count * GROUP_W) * pool_scale).astype(BF16)
    mixer_out = jnp.dot(mapped, w_out, preferred_element_type=F32) * jax.nn.sigmoid(
        gate_logit.astype(F32)
    )
    mixed = ALPHA * residual.astype(F32) + mixer_out

    quarters = [
        lax.dynamic_slice_in_dim(mixed, (j ^ k) * quarter, quarter, 0) for k in range(tp)
    ]
    scales = jnp.pad(
        jnp.stack([first_gain, first_bias, second_gain, second_bias]), ((0, 4), (0, 0))
    )
    both = [jnp.concatenate([q, scales]) for q in quarters]
    both = [both[0]] + [swap_with(both[k], "tp", k) for k in range(1, tp)]
    tokens, normed_rel, gains = first_norm(place, both, quarter)

    down_own, tokens = lax.optimization_barrier((w_down[0], tokens))
    first_w, down_w = weight_parts(w_gate[0], w_up[0], down_own, tp)

    everyone = line_gather(tokens, "sp")
    inputs, first_hidden = hidden_units(everyone, first_w[0])
    hidden_rel = [first_hidden] + [
        hidden_units([inputs], first_w[k])[1] for k in range(1, tp)
    ]

    final_rel = []
    half_rows = (sp // 2) * quarter
    for k in range(tp):
        partial = weighted_outputs(place, share, hidden_rel, down_w[k])
        other = swap_with(partial[half_rows:], "sp", 1)
        joined = partial[:half_rows].astype(F32) + other.astype(F32)
        moe = joined[:quarter]
        sent = joined.astype(BF16)
        for d in range(1, sp // 2):
            got = swap_with(sent[d * quarter : (d + 1) * quarter], "sp", 2 * d)
            moe = moe + got.astype(F32)
        final_rel.append(ALPHA * normed_rel[k].astype(F32) + moe)
    out_rel = [
        (r * gains[k][2] + gains[k][3]).astype(BF16)
        for k, r in enumerate(norm_rows(final_rel, features))
    ]
    home_rel = [out_rel[0]] + [swap_with(out_rel[k], "tp", k) for k in range(1, tp)]
    return jnp.concatenate(in_order(home_rel, j))


def solution(mesh):
    return jax.shard_map(
        body,
        mesh=mesh,
        in_specs=(
            P("tp", "sp"),
            P("sp"),
            P(),
            P(),
            P(None, "tp"),
            P("sp", "tp"),
            P("sp", "tp"),
            P("tp"),
            P("tp"),
            P("sp", None),
            P("sp", None),
            P("sp", None, "tp"),
            P("sp", None, "tp"),
            P("sp", None, "tp"),
            P("tp"),
            P("tp"),
        ),
        out_specs=P("sp", "tp"),
        check_vma=False,
    )
```

```python
import functools

import jax
import jax.numpy as jnp
from jax import lax
from jax.experimental import pallas as pl
from jax.experimental.pallas import tpu as pltpu
from jax.sharding import PartitionSpec as P


GROUP_W = 64
EPS = 1e-05
ALPHA = 8.0**0.25
HALO = 16
F32 = jnp.float32
BF16 = jnp.bfloat16


def swap_with(part, axis, bits):
    size = lax.axis_size(axis)
    return lax.ppermute(part, axis, [(i, i ^ bits) for i in range(size)])


def in_order(relative, index):
    stacked = jnp.stack(relative)
    return [
        lax.dynamic_index_in_dim(stacked, index ^ p, 0, keepdims=False)
        for p in range(len(relative))
    ]


def exchange_all(part, axis):
    return [part] + [swap_with(part, axis, k) for k in range(1, lax.axis_size(axis))]


def line_gather(part, axis):
    size = lax.axis_size(axis)
    mine = [part]
    for k in range(1, size // 2):
        mine.append(swap_with(part, axis, 2 * k))
    return mine + [swap_with(m, axis, 1) for m in mine]


TABLE = HALO + 8


def table_kernel(x_ref, docs_ref, table_ref):
    channels, positions = x_ref.shape
    docs = docs_ref[...].astype(F32).reshape(1, positions)
    last_doc = docs[:, positions - 1 :]
    ending = jnp.where(docs == last_doc, 1.0, 0.0)
    length = jnp.sum(ending, axis=1, keepdims=True)
    row = lax.broadcasted_iota(jnp.int32, (TABLE, positions), 0)
    col = lax.broadcasted_iota(jnp.int32, (TABLE, positions), 1)
    pick = jnp.where(col == positions - HALO + row, 1.0, 0.0)
    pick = jnp.where(row == HALO, jnp.broadcast_to(ending, pick.shape), pick)
    got = lax.dot_general(
        pick.astype(BF16), x_ref[...], (((1,), (1,)), ((), ())), preferred_element_type=F32
    )
    row = lax.broadcasted_iota(jnp.int32, (TABLE, channels), 0)
    got = jnp.where(row == HALO + 1, last_doc, got)
    table_ref[...] = jnp.where(row == HALO + 2, length, got)


def starts_of(docs_ref, positions):
    docs = jnp.broadcast_to(docs_ref[...].reshape(1, positions), (8, positions))
    lane = lax.broadcasted_iota(jnp.int32, (8, positions), 1)
    opens = (docs != pltpu.roll(docs, 1, 1)) & (lane > 0)
    start = jnp.where(opens, lane, 0)
    step = 1
    while step < positions:
        moved = pltpu.roll(start, step, 1)
        start = jnp.maximum(start, jnp.where(lane >= step, moved, 0))
        step *= 2
    return start


def units_of(channels, j):
    unit = min(GROUP_W, channels)
    for u in range(channels // unit):
        group = (j * channels + u * unit) // GROUP_W
        yield slice(u * unit, (u + 1) * unit), group % 2 == 1, lax.shift_left(2, group // 2 % 4)


def local_kernel(place_ref, x_ref, docs_ref, sum_ref, start_ref):
    channels, positions = x_ref.shape
    start_ref[...] = starts_of(docs_ref, positions)
    s_at = lax.broadcasted_iota(jnp.int32, (positions, positions), 0)
    t_at = lax.broadcasted_iota(jnp.int32, (positions, positions), 1)
    for rows, whole_doc, window in units_of(channels, place_ref[1]):
        reach = jnp.where(whole_doc, positions, window)
        lower = jnp.maximum(start_ref[:1, :], t_at[:1, :] + 1 - reach)
        mask = (s_at >= lower) & (s_at <= t_at)
        sum_ref[rows, :] = jnp.dot(
            x_ref[rows, :], mask.astype(BF16), preferred_element_type=F32
        )


def pooled_kernel(place_ref, x_ref, docs_ref, start_ref, sum_ref, *rest):
    *table_refs, out_ref = rest
    channels, positions = x_ref.shape
    i, j = place_ref[0], place_ref[1]
    first_doc = docs_ref[...].astype(F32).reshape(1, positions)[:, :1]
    before = jnp.zeros((TABLE, channels), F32)
    carried = jnp.zeros((TABLE, channels), F32)
    near_ref, *far_refs = table_refs
    for k in range(1, 2 * len(table_refs)):
        table = near_ref[...] if k == 1 else far_refs[k // 2 - 1][k % 2]
        earlier = jnp.where((i ^ k) < i, 1.0, 0.0)
        previous = jnp.where((i ^ k) == i - 1, 1.0, 0.0)
        same = jnp.where(table[HALO + 1 : HALO + 2, :1] == first_doc, earlier, 0.0)
        carried = carried + same * table
        before = before + previous * table
    count = carried[HALO + 2 : HALO + 3, :1]
    t_at = lax.broadcasted_iota(jnp.int32, (1, positions), 1)
    start = start_ref[:1, :]
    in_first = jnp.where(start == 0, 1.0, 0.0)
    doc_count = (t_at + 1 - start).astype(F32) + in_first * count
    row = lax.broadcasted_iota(jnp.int32, (TABLE, channels), 0)
    carry_row = jnp.where(row == HALO, carried, 0.0)
    over_first = jnp.broadcast_to(in_first, (TABLE, positions))
    carry = lax.dot_general(
        carry_row,
        over_first,
        (((0,), (0,)), ((), ())),
        precision=lax.Precision.HIGHEST,
        preferred_element_type=F32,
    )
    h_at = lax.broadcasted_iota(jnp.int32, (TABLE, positions), 0) - HALO
    reached = jnp.where(h_at.astype(F32) >= -count, over_first, 0.0)
    reached = jnp.where(h_at < 0, reached, 0.0)
    for rows, whole_doc, window in units_of(channels, j):
        halo_mask = jnp.where(h_at >= t_at + 1 - window, reached, 0.0)
        halo = lax.dot_general(
            before.astype(BF16),
            halo_mask.astype(BF16),
            (((0,), (0,)), ((), ())),
            preferred_element_type=F32,
        )
        whole = jnp.where(whole_doc, 1.0, 0.0)
        total = sum_ref[rows, :] + whole * carry[rows] + (1.0 - whole) * halo[rows]
        most = jnp.where(whole_doc, float(1 << 30), window.astype(F32))
        total = total / jnp.minimum(doc_count, most)
        out_ref[rows, :] = (total - x_ref[rows, :].astype(F32)).astype(BF16)


def in_vmem(count):
    return [pl.BlockSpec(memory_space=pltpu.VMEM)] * count


def room(mebibytes):
    return pltpu.CompilerParams(vmem_limit_bytes=mebibytes << 20)


def pooled_channels(pool_in, doc_ids, place):
    channels, positions = pool_in.shape
    scalars = pl.BlockSpec(memory_space=pltpu.SMEM)
    table = pl.pallas_call(
        table_kernel,
        out_shape=jax.ShapeDtypeStruct((TABLE, channels), F32),
        in_specs=in_vmem(2),
        out_specs=in_vmem(1)[0],
        compiler_params=room(4),
        name="table",
    )(pool_in, doc_ids)
    near = swap_with(table, "sp", 1)
    pair = jnp.stack([table, near])
    sums, start = pl.pallas_call(
        local_kernel,
        out_shape=(
            jax.ShapeDtypeStruct((channels, positions), F32),
            jax.ShapeDtypeStruct((8, positions), jnp.int32),
        ),
        in_specs=[scalars] + in_vmem(2),
        out_specs=tuple(in_vmem(2)),
        compiler_params=room(8),
        name="local",
    )(place, pool_in, doc_ids)
    far = [swap_with(pair, "sp", 2 * k) for k in range(1, lax.axis_size("sp") // 2)]
    return pl.pallas_call(
        pooled_kernel,
        out_shape=jax.ShapeDtypeStruct((channels, positions), BF16),
        in_specs=[scalars] + in_vmem(5 + len(far)),
        out_specs=in_vmem(1)[0],
        compiler_params=room(8),
        name="pooled",
    )(place, pool_in, doc_ids, start, sums, near, *far)


def gather_rows_kernel(*refs):
    *parts, out_ref = refs
    rows = parts[0].shape[0]
    for p, part in enumerate(parts):
        out_ref[p * rows : (p + 1) * rows, :] = part[...]


def hidden_kernel(count, *refs):
    row_refs, weights, outs = refs[:count], refs[count:-1], refs[-1:]
    if count > 1:
        weights, outs = refs[count:-2], refs[-2:]
        gather_rows_kernel(*row_refs, outs[0])
    rows = outs[0] if count > 1 else row_refs[0]
    if len(weights) == 1:
        both = jnp.dot(rows[...], weights[0][...], preferred_element_type=F32)
        half = both.shape[1] // 2
        gated, up = both[:, :half], both[:, half:]
    else:
        gated, up = (
            jnp.dot(rows[...], w[...], preferred_element_type=F32) for w in weights
        )
    outs[-1][...] = (gated * jax.nn.sigmoid(gated) * up).astype(BF16)


def hidden_units(row_parts, weights):
    count = len(row_parts)
    rows = sum(r.shape[0] for r in row_parts)
    wide = sum(w.shape[1] for w in weights) // 2
    shape = jax.ShapeDtypeStruct((rows, wide), BF16)
    joined = jax.ShapeDtypeStruct((rows, row_parts[0].shape[1]), BF16)
    outs = (joined, shape) if count > 1 else (shape,)
    got = pl.pallas_call(
        functools.partial(hidden_kernel, count),
        out_shape=outs,
        in_specs=in_vmem(count + len(weights)),
        out_specs=tuple(in_vmem(len(outs))),
        compiler_params=room(20),
        name="hidden",
    )(*row_parts, *weights)
    return (got[0], got[-1])


def stage_kernel(*refs):
    parts = len(refs) // 3
    for k in range(parts):
        half = refs[2 * k].shape[1]
        refs[2 * parts + k][:, :half] = refs[2 * k][...]
        refs[2 * parts + k][:, half:] = refs[2 * k + 1][...]


def staged(pairs):
    flat = [w for pair in pairs for w in pair]
    return pl.pallas_call(
        stage_kernel,
        out_shape=tuple(
            jax.ShapeDtypeStruct((g.shape[0], 2 * g.shape[1]), BF16) for g, _ in pairs
        ),
        in_specs=in_vmem(len(flat)),
        out_specs=tuple(in_vmem(len(pairs))),
        compiler_params=room(16),
        name="stage",
    )(*flat)


def down_kernel(parts, place_ref, share_ref, *refs):
    hidden, weights, out_ref = refs[:parts], refs[parts:-1], refs[-1]
    depth, at = hidden[0].shape[1], 0
    for weight in weights:
        total = None
        for k in range(parts):
            rows = pl.ds(pl.multiple_of((place_ref[1] ^ k) * depth, depth), depth)
            piece = jnp.dot(hidden[k][...], weight[rows, :], preferred_element_type=F32)
            total = piece if total is None else total + piece
        wide = weight.shape[1]
        out_ref[:, at : at + wide] = (total * share_ref[...]).astype(BF16)
        at += wide


def weighted_outputs(place, share, hidden, weights):
    wide = sum(w.shape[1] for w in weights)
    return pl.pallas_call(
        functools.partial(down_kernel, len(hidden)),
        out_shape=jax.ShapeDtypeStruct((hidden[0].shape[0], wide), BF16),
        in_specs=[pl.BlockSpec(memory_space=pltpu.SMEM)]
        + in_vmem(1 + len(hidden) + len(weights)),
        out_specs=in_vmem(1)[0],
        compiler_params=room(14),
        name="down",
    )(place, share, *hidden, *weights)


def first_norm_kernel(parts, place_ref, *refs):
    rows, (tokens_ref, normed_ref, scale_ref) = refs[:parts], refs[parts:]
    count, wide = normed_ref.shape[1:]
    total = square = 0.0
    for ref in rows:
        part = ref[:count, :]
        total = total + jnp.sum(part, axis=1, keepdims=True)
        square = square + jnp.sum(part * part, axis=1, keepdims=True)
    mean = total / (parts * wide)
    scale = lax.rsqrt(square / (parts * wide) - mean * mean + EPS)
    for k, ref in enumerate(rows):
        gains = ref[count:, :]
        scale_ref[k] = gains
        part = (ref[:count, :] - mean) * scale * gains[:1] + gains[1:2]
        part = part.astype(BF16)
        normed_ref[k] = part
        at = pl.multiple_of((place_ref[1] ^ k) * wide, wide)
        tokens_ref[:, pl.ds(at, wide)] = part


def first_norm(place, rows, count):
    parts, wide = len(rows), rows[0].shape[1]
    tokens, normed, scales = pl.pallas_call(
        functools.partial(first_norm_kernel, parts),
        out_shape=(
            jax.ShapeDtypeStruct((count, parts * wide), BF16),
            jax.ShapeDtypeStruct((parts, count, wide), BF16),
            jax.ShapeDtypeStruct((parts, rows[0].shape[0] - count, wide), F32),
        ),
        in_specs=[pl.BlockSpec(memory_space=pltpu.SMEM)] + in_vmem(parts),
        out_specs=tuple(in_vmem(3)),
        compiler_params=room(8),
        name="norm",
    )(place, *rows)
    return tokens, normed, scales


def share_kernel(place_ref, *refs):
    *tables, out_ref = refs
    count = tables[0].shape[-1]
    mine = place_ref[0].astype(F32)
    rows = []
    for core in range(2):
        for table in tables:
            chosen = jnp.where(table[core, 0] == mine, table[core, 1], 0.0)
            rows.append(jnp.sum(chosen, axis=0, keepdims=True))
    rows = jnp.concatenate(rows)
    row = lax.broadcasted_iota(jnp.int32, (count, count), 0)
    col = lax.broadcasted_iota(jnp.int32, (count, count), 1)
    columns = lax.dot_general(
        jnp.where(row == col, 1.0, 0.0),
        rows,
        (((1,), (1,)), ((), ())),
        precision=lax.Precision.HIGHEST,
        preferred_element_type=F32,
    )
    for slot in range(rows.shape[0]):
        out_ref[slot * count : (slot + 1) * count, :] = columns[:, slot : slot + 1]


def token_shares(place, tables):
    slots, count = 2 * len(tables), tables[0].shape[-1]
    return pl.pallas_call(
        share_kernel,
        out_shape=jax.ShapeDtypeStruct((slots * count, 1), F32),
        in_specs=[pl.BlockSpec(memory_space=pltpu.SMEM)] + in_vmem(len(tables)),
        out_specs=in_vmem(1)[0],
        compiler_params=room(4),
        name="share",
    )(place, *tables)


def last_norm_kernel(parts, arrange, normed_ref, scale_ref, *refs):
    outs, refs = refs[-parts:], refs[:-parts]
    each = len(refs) // parts
    sums = []
    for k in range(parts):
        own, *others = refs[k * each : (k + 1) * each]
        total = own[...]
        for other in others:
            total = total + other[...].astype(F32)
        sums.append(total)
    rows = [
        ALPHA * normed_ref[k].astype(F32) + part for k, part in enumerate(arrange(*sums))
    ]
    features = sum(r.shape[1] for r in rows)
    mean = sum(jnp.sum(r, axis=1, keepdims=True) for r in rows) / features
    square = sum(jnp.sum(r * r, axis=1, keepdims=True) for r in rows) / features
    scale = lax.rsqrt(square - mean * mean + EPS)
    for k, out_ref in enumerate(outs):
        part = (rows[k] - mean) * scale * scale_ref[k, 2:3, :] + scale_ref[k, 3:4, :]
        out_ref[...] = part.astype(BF16)


def last_norm(arrange, normed, scales, groups):
    parts, count, wide = normed.shape
    flat = [r for group in groups for r in group]
    return pl.pallas_call(
        functools.partial(last_norm_kernel, parts, arrange),
        out_shape=tuple(jax.ShapeDtypeStruct((count, wide), BF16) for _ in groups),
        in_specs=in_vmem(2 + len(flat)),
        out_specs=tuple(in_vmem(parts)),
        compiler_params=room(12),
        name="last",
    )(normed, scales, *flat)


def weight_parts(w_gate, w_up, w_down, tp):
    if tp != 4:
        gate, up, down = (exchange_all(w, "tp") for w in (w_gate, w_up, w_down))
        pairs = [list(pair) for pair in zip(gate, up)]
        return pairs, [[w] for w in down], lambda *parts: list(parts)
    gate1 = swap_with(w_gate, "tp", 1)
    up2 = swap_with(w_up, "tp", 2)
    up1 = swap_with(w_up, "tp", 1)
    gate2 = swap_with(w_gate, "tp", 2)
    up3 = swap_with(up2, "tp", 1)
    gate3 = swap_with(gate1, "tp", 2)
    wide = w_down.shape[1] // 2
    left, right = w_down[:, :wide], w_down[:, wide:]
    down1_left = swap_with(left, "tp", 1)
    down2_right = swap_with(right, "tp", 2)
    down1_right = swap_with(right, "tp", 1)
    down2_left = swap_with(left, "tp", 2)
    down3_right = swap_with(down2_right, "tp", 1)
    down3_left = swap_with(down1_left, "tp", 2)
    near = staged([(w_gate, w_up), (gate1, up1), (gate2, up2)])
    first = [[w] for w in near] + [[gate3, up3]]
    down = [
        [w_down],
        [down1_left, down2_right],
        [down1_right, down2_left],
        [down3_left, down3_right],
    ]

    def by_distance(own, early, late, last):
        one = jnp.concatenate([early[:, :wide], late[:, :wide]], axis=1)
        two = jnp.concatenate([late[:, wide:], early[:, wide:]], axis=1)
        return [own, one, two, last]

    return first, down, by_distance


def body(
    pool_in,
    doc_ids,
    pool_map,
    pool_scale,
    w_out,
    gate_logit,
    residual,
    first_gain,
    first_bias,
    routes,
    route_weight,
    w_gate,
    w_up,
    w_down,
    second_gain,
    second_bias,
):
    sp, tp = lax.axis_size("sp"), lax.axis_size("tp")
    i, j = lax.axis_index("sp"), lax.axis_index("tp")
    _, positions = pool_in.shape
    quarter = positions // tp

    place = jnp.stack([i, j])
    pooled = pooled_channels(pool_in, doc_ids, place)
    pooled_rel = exchange_all(pooled, "tp")
    my_routes = lax.dynamic_slice_in_dim(routes, j * quarter, quarter, 0)
    my_weights = lax.dynamic_slice_in_dim(route_weight, j * quarter, quarter, 0)
    chosen = jnp.stack([my_routes.astype(F32).T, my_weights.T])
    chosen = jnp.stack([chosen, swap_with(chosen, "sp", 1)])
    chosen = [chosen] + [swap_with(chosen, "sp", 2 * k) for k in range(1, sp // 2)]
    share = token_shares(place, chosen)

    gathered = jnp.concatenate(in_order(pooled_rel, j))
    group_count = gathered.shape[0] // GROUP_W
    grouped = jnp.einsum(
        "gct,gcd->tgd",
        gathered.reshape(group_count, GROUP_W, positions),
        pool_map,
        preferred_element_type=F32,
    )
    mapped = (grouped.reshape(positions, group_count * GROUP_W) * pool_scale).astype(BF16)
    mixer_out = jnp.dot(mapped, w_out, preferred_element_type=F32) * jax.nn.sigmoid(
        gate_logit.astype(F32)
    )
    mixed = ALPHA * residual.astype(F32) + mixer_out

    quarters = [
        lax.dynamic_slice_in_dim(mixed, (j ^ k) * quarter, quarter, 0) for k in range(tp)
    ]
    scales = jnp.pad(
        jnp.stack([first_gain, first_bias, second_gain, second_bias]), ((0, 4), (0, 0))
    )
    both = [jnp.concatenate([q, scales]) for q in quarters]
    both = [both[0]] + [swap_with(both[k], "tp", k) for k in range(1, tp)]
    tokens, normed, scales = first_norm(place, both, quarter)

    down_own, tokens = lax.optimization_barrier((w_down[0], tokens))
    first_w, down_w, by_distance = weight_parts(w_gate[0], w_up[0], down_own, tp)

    everyone = line_gather(tokens, "sp")
    inputs, first_hidden = hidden_units(everyone, first_w[0])
    hidden_rel = [first_hidden] + [
        hidden_units([inputs], first_w[k])[1] for k in range(1, tp)
    ]

    groups = []
    half_rows = (sp // 2) * quarter
    for k in range(tp):
        partial = weighted_outputs(place, share, hidden_rel, down_w[k])
        other = swap_with(partial[half_rows:], "sp", 1)
        joined = partial[:half_rows].astype(F32) + other.astype(F32)
        sent = joined.astype(BF16)
        got = [
            swap_with(sent[d * quarter : (d + 1) * quarter], "sp", 2 * d)
            for d in range(1, sp // 2)
        ]
        groups.append([joined[:quarter]] + got)
    out_rel = last_norm(by_distance, normed, scales, groups)
    home_rel = [out_rel[0]] + [swap_with(out_rel[k], "tp", k) for k in range(1, tp)]
    return jnp.concatenate(in_order(home_rel, j))


def solution(mesh):
    return jax.shard_map(
        body,
        mesh=mesh,
        in_specs=(
            P("tp", "sp"),
            P("sp"),
            P(),
            P(),
            P(None, "tp"),
            P("sp", "tp"),
            P("sp", "tp"),
            P("tp"),
            P("tp"),
            P("sp", None),
            P("sp", None),
            P("sp", None, "tp"),
            P("sp", None, "tp"),
            P("sp", None, "tp"),
            P("tp"),
            P("tp"),
        ),
        out_specs=P("sp", "tp"),
        check_vma=False,
    )
```

```python
import functools

import jax
import jax.numpy as jnp
from jax import lax
from jax.experimental import pallas as pl
from jax.experimental.pallas import tpu as pltpu
from jax.sharding import PartitionSpec as P


GROUP_W = 64
EPS = 1e-05
ALPHA = 8.0**0.25
HALO = 16
F32 = jnp.float32
BF16 = jnp.bfloat16


def swap_with(part, axis, bits):
    size = lax.axis_size(axis)
    return lax.ppermute(part, axis, [(i, i ^ bits) for i in range(size)])


def in_order(relative, index):
    stacked = jnp.stack(relative)
    return [
        lax.dynamic_index_in_dim(stacked, index ^ p, 0, keepdims=False)
        for p in range(len(relative))
    ]


def exchange_all(part, axis):
    return [part] + [swap_with(part, axis, k) for k in range(1, lax.axis_size(axis))]


def line_gather(part, axis):
    size = lax.axis_size(axis)
    mine = [part]
    for k in range(1, size // 2):
        mine.append(swap_with(part, axis, 2 * k))
    return mine + [swap_with(m, axis, 1) for m in mine]


TABLE = HALO + 8


def table_kernel(x_ref, docs_ref, table_ref):
    channels, positions = x_ref.shape
    docs = docs_ref[...].astype(F32).reshape(1, positions)
    last_doc = docs[:, positions - 1 :]
    ending = jnp.where(docs == last_doc, 1.0, 0.0)
    length = jnp.sum(ending, axis=1, keepdims=True)
    row = lax.broadcasted_iota(jnp.int32, (TABLE, positions), 0)
    col = lax.broadcasted_iota(jnp.int32, (TABLE, positions), 1)
    pick = jnp.where(col == positions - HALO + row, 1.0, 0.0)
    pick = jnp.where(row == HALO, jnp.broadcast_to(ending, pick.shape), pick)
    got = lax.dot_general(
        pick.astype(BF16), x_ref[...], (((1,), (1,)), ((), ())), preferred_element_type=F32
    )
    row = lax.broadcasted_iota(jnp.int32, (TABLE, channels), 0)
    got = jnp.where(row == HALO + 1, last_doc, got)
    table_ref[...] = jnp.where(row == HALO + 2, length, got)


def starts_of(docs_ref, positions):
    docs = jnp.broadcast_to(docs_ref[...].reshape(1, positions), (8, positions))
    lane = lax.broadcasted_iota(jnp.int32, (8, positions), 1)
    opens = (docs != pltpu.roll(docs, 1, 1)) & (lane > 0)
    start = jnp.where(opens, lane, 0)
    step = 1
    while step < positions:
        moved = pltpu.roll(start, step, 1)
        start = jnp.maximum(start, jnp.where(lane >= step, moved, 0))
        step *= 2
    return start


def units_of(channels, j):
    unit = min(GROUP_W, channels)
    for u in range(channels // unit):
        group = (j * channels + u * unit) // GROUP_W
        yield slice(u * unit, (u + 1) * unit), group % 2 == 1, lax.shift_left(2, group // 2 % 4)


def local_kernel(place_ref, x_ref, docs_ref, sum_ref, start_ref):
    channels, positions = x_ref.shape
    start_ref[...] = starts_of(docs_ref, positions)
    s_at = lax.broadcasted_iota(jnp.int32, (positions, positions), 0)
    t_at = lax.broadcasted_iota(jnp.int32, (positions, positions), 1)
    for rows, whole_doc, window in units_of(channels, place_ref[1]):
        reach = jnp.where(whole_doc, positions, window)
        lower = jnp.maximum(start_ref[:1, :], t_at[:1, :] + 1 - reach)
        mask = (s_at >= lower) & (s_at <= t_at)
        sum_ref[rows, :] = jnp.dot(
            x_ref[rows, :], mask.astype(BF16), preferred_element_type=F32
        )


def pooled_kernel(place_ref, x_ref, docs_ref, start_ref, sum_ref, *rest):
    *table_refs, out_ref = rest
    channels, positions = x_ref.shape
    i, j = place_ref[0], place_ref[1]
    first_doc = docs_ref[...].astype(F32).reshape(1, positions)[:, :1]
    before = jnp.zeros((TABLE, channels), F32)
    carried = jnp.zeros((TABLE, channels), F32)
    near_ref, *far_refs = table_refs
    for k in range(1, 2 * len(table_refs)):
        table = near_ref[...] if k == 1 else far_refs[k // 2 - 1][k % 2]
        earlier = jnp.where((i ^ k) < i, 1.0, 0.0)
        previous = jnp.where((i ^ k) == i - 1, 1.0, 0.0)
        same = jnp.where(table[HALO + 1 : HALO + 2, :1] == first_doc, earlier, 0.0)
        carried = carried + same * table
        before = before + previous * table
    count = carried[HALO + 2 : HALO + 3, :1]
    t_at = lax.broadcasted_iota(jnp.int32, (1, positions), 1)
    start = start_ref[:1, :]
    in_first = jnp.where(start == 0, 1.0, 0.0)
    doc_count = (t_at + 1 - start).astype(F32) + in_first * count
    row = lax.broadcasted_iota(jnp.int32, (TABLE, channels), 0)
    carry_row = jnp.where(row == HALO, carried, 0.0)
    over_first = jnp.broadcast_to(in_first, (TABLE, positions))
    carry = lax.dot_general(
        carry_row,
        over_first,
        (((0,), (0,)), ((), ())),
        precision=lax.Precision.HIGHEST,
        preferred_element_type=F32,
    )
    h_at = lax.broadcasted_iota(jnp.int32, (TABLE, positions), 0) - HALO
    reached = jnp.where(h_at.astype(F32) >= -count, over_first, 0.0)
    reached = jnp.where(h_at < 0, reached, 0.0)
    for rows, whole_doc, window in units_of(channels, j):
        halo_mask = jnp.where(h_at >= t_at + 1 - window, reached, 0.0)
        halo = lax.dot_general(
            before.astype(BF16),
            halo_mask.astype(BF16),
            (((0,), (0,)), ((), ())),
            preferred_element_type=F32,
        )
        whole = jnp.where(whole_doc, 1.0, 0.0)
        total = sum_ref[rows, :] + whole * carry[rows] + (1.0 - whole) * halo[rows]
        most = jnp.where(whole_doc, float(1 << 30), window.astype(F32))
        total = total / jnp.minimum(doc_count, most)
        out_ref[rows, :] = (total - x_ref[rows, :].astype(F32)).astype(BF16)


def in_vmem(count):
    return [pl.BlockSpec(memory_space=pltpu.VMEM)] * count


def room(mebibytes):
    return pltpu.CompilerParams(vmem_limit_bytes=mebibytes << 20)


def table_call(pool_in, doc_ids):
    return pl.pallas_call(
        table_kernel,
        out_shape=jax.ShapeDtypeStruct((TABLE, pool_in.shape[0]), F32),
        in_specs=in_vmem(2),
        out_specs=in_vmem(1)[0],
        compiler_params=room(4),
        name="table",
    )(pool_in, doc_ids)


def pooled_channels(pool_in, doc_ids, place):
    channels, positions = pool_in.shape
    scalars = pl.BlockSpec(memory_space=pltpu.SMEM)
    table = table_call(pool_in, doc_ids)
    near = swap_with(table, "sp", 1)
    pair = jnp.stack([table, near])
    sums, start = pl.pallas_call(
        local_kernel,
        out_shape=(
            jax.ShapeDtypeStruct((channels, positions), F32),
            jax.ShapeDtypeStruct((8, positions), jnp.int32),
        ),
        in_specs=[scalars] + in_vmem(2),
        out_specs=tuple(in_vmem(2)),
        compiler_params=room(8),
        name="local",
    )(place, pool_in, doc_ids)
    far = [swap_with(pair, "sp", 2 * k) for k in range(1, lax.axis_size("sp") // 2)]
    return pl.pallas_call(
        pooled_kernel,
        out_shape=jax.ShapeDtypeStruct((channels, positions), BF16),
        in_specs=[scalars] + in_vmem(5 + len(far)),
        out_specs=in_vmem(1)[0],
        compiler_params=room(8),
        name="pooled",
    )(place, pool_in, doc_ids, start, sums, near, *far)


def gather_rows_kernel(*refs):
    *parts, out_ref = refs
    rows = parts[0].shape[0]
    for p, part in enumerate(parts):
        out_ref[p * rows : (p + 1) * rows, :] = part[...]


def hidden_kernel(count, *refs):
    row_refs, weights, outs = refs[:count], refs[count:-1], refs[-1:]
    if count > 1:
        weights, outs = refs[count:-2], refs[-2:]
        gather_rows_kernel(*row_refs, outs[0])
    rows = outs[0] if count > 1 else row_refs[0]
    if len(weights) == 1:
        both = jnp.dot(rows[...], weights[0][...], preferred_element_type=F32)
        half = both.shape[1] // 2
        gated, up = both[:, :half], both[:, half:]
    else:
        gated, up = (
            jnp.dot(rows[...], w[...], preferred_element_type=F32) for w in weights
        )
    outs[-1][...] = (gated * jax.nn.sigmoid(gated) * up).astype(BF16)


def hidden_units(row_parts, weights):
    count = len(row_parts)
    rows = sum(r.shape[0] for r in row_parts)
    wide = sum(w.shape[1] for w in weights) // 2
    shape = jax.ShapeDtypeStruct((rows, wide), BF16)
    joined = jax.ShapeDtypeStruct((rows, row_parts[0].shape[1]), BF16)
    outs = (joined, shape) if count > 1 else (shape,)
    got = pl.pallas_call(
        functools.partial(hidden_kernel, count),
        out_shape=outs,
        in_specs=in_vmem(count + len(weights)),
        out_specs=tuple(in_vmem(len(outs))),
        compiler_params=room(20),
        name="hidden",
    )(*row_parts, *weights)
    return (got[0], got[-1])


def stage_kernel(pieces, *refs):
    at = 0
    outs = refs[sum(sum(p) for p in pieces) :]
    for out, pair in zip(outs, pieces):
        half = out.shape[1] // 2
        for side, count in enumerate(pair):
            row = 0
            for ref in refs[at : at + count]:
                depth = ref.shape[0]
                out[row : row + depth, side * half : (side + 1) * half] = ref[...]
                row += depth
            at += count


def staged(pairs):
    flat = [w for pair in pairs for side in pair for w in side]
    pieces = tuple(tuple(len(side) for side in pair) for pair in pairs)
    depth = sum(w.shape[0] for w in pairs[0][0])
    return pl.pallas_call(
        functools.partial(stage_kernel, pieces),
        out_shape=tuple(
            jax.ShapeDtypeStruct((depth, 2 * pair[0][0].shape[1]), BF16) for pair in pairs
        ),
        in_specs=in_vmem(len(flat)),
        out_specs=tuple(in_vmem(len(pairs))),
        compiler_params=room(16),
        name="stage",
    )(*flat)


def down_kernel(parts, place_ref, share_ref, *refs):
    hidden, weights, out_ref = refs[:parts], refs[parts:-1], refs[-1]
    depth, total = hidden[0].shape[1], None
    for k in range(parts):
        rows = pl.ds(pl.multiple_of((place_ref[1] ^ k) * depth, depth), depth)
        near = [weight[rows, :] for weight in weights]
        near = near[0] if len(near) == 1 else jnp.concatenate(near, axis=1)
        piece = jnp.dot(hidden[k][...], near, preferred_element_type=F32)
        total = piece if total is None else total + piece
    out_ref[...] = (total * share_ref[...]).astype(BF16)


def weighted_outputs(place, share, hidden, weights):
    wide = sum(w.shape[1] for w in weights)
    return pl.pallas_call(
        functools.partial(down_kernel, len(hidden)),
        out_shape=jax.ShapeDtypeStruct((hidden[0].shape[0], wide), BF16),
        in_specs=[pl.BlockSpec(memory_space=pltpu.SMEM)]
        + in_vmem(1 + len(hidden) + len(weights)),
        out_specs=in_vmem(1)[0],
        compiler_params=room(14),
        name="down",
    )(place, share, *hidden, *weights)


LANES = 128


def rows_kernel(place_ref, mixed_ref, *outs):
    count, wide = outs[0].shape[0], mixed_ref.shape[1]
    lane = lax.broadcasted_iota(jnp.int32, (count, LANES), 1)
    for k, out_ref in enumerate(outs):
        at = pl.multiple_of((place_ref[1] ^ k) * count, 8)
        part = mixed_ref[pl.ds(at, count), :]
        mean = jnp.sum(part, axis=1, keepdims=True) / wide
        out_ref[:, :wide] = (part - mean).astype(BF16)
        high = mean.astype(BF16).astype(F32)
        middle = (mean - high).astype(BF16).astype(F32)
        low = mean - high - middle
        terms = jnp.where(lane == 0, high, jnp.where(lane == 1, middle, low))
        out_ref[:, wide:] = terms.astype(BF16)


def rows_to_send(place, mixed, parts):
    count, wide = mixed.shape[0] // parts, mixed.shape[1]
    return pl.pallas_call(
        rows_kernel,
        out_shape=tuple(
            jax.ShapeDtypeStruct((count, wide + LANES), BF16) for _ in range(parts)
        ),
        in_specs=[pl.BlockSpec(memory_space=pltpu.SMEM)] + in_vmem(1),
        out_specs=tuple(in_vmem(parts)),
        compiler_params=room(4),
        name="rows",
    )(place, mixed)


def first_norm_kernel(parts, place_ref, *refs):
    rows, gains, outs = refs[:parts], refs[parts : 2 * parts], refs[2 * parts :]
    tokens_ref, normed_ref, scale_ref = outs
    wide = normed_ref.shape[2]
    values = []
    for ref in rows:
        mean = ref[:, wide : wide + 3].astype(F32)
        mean = mean[:, :1] + mean[:, 1:2] + mean[:, 2:3]
        values.append(ref[:, :wide].astype(F32) + mean)
    features = parts * wide
    mean = sum(jnp.sum(v, axis=1, keepdims=True) for v in values) / features
    square = sum(jnp.sum(v * v, axis=1, keepdims=True) for v in values) / features
    scale = lax.rsqrt(square - mean * mean + EPS)
    for k, value in enumerate(values):
        scale_ref[k] = gains[k][...]
        part = (value - mean) * scale * gains[k][:1, :] + gains[k][1:2, :]
        part = part.astype(BF16)
        normed_ref[k] = part
        at = pl.multiple_of((place_ref[1] ^ k) * wide, wide)
        tokens_ref[:, pl.ds(at, wide)] = part


def first_norm(place, rows, gains):
    parts, count = len(rows), rows[0].shape[0]
    wide = gains[0].shape[1]
    return pl.pallas_call(
        functools.partial(first_norm_kernel, parts),
        out_shape=(
            jax.ShapeDtypeStruct((count, parts * wide), BF16),
            jax.ShapeDtypeStruct((parts, count, wide), BF16),
            jax.ShapeDtypeStruct((parts,) + gains[0].shape, F32),
        ),
        in_specs=[pl.BlockSpec(memory_space=pltpu.SMEM)] + in_vmem(2 * parts),
        out_specs=tuple(in_vmem(3)),
        compiler_params=room(8),
        name="norm",
    )(place, *rows, *gains)


def share_kernel(place_ref, *refs):
    *tables, out_ref = refs
    count = tables[0].shape[-1]
    mine = place_ref[0].astype(F32)
    rows = []
    for core in range(2):
        for table in tables:
            chosen = jnp.where(table[core, 0] == mine, table[core, 1], 0.0)
            rows.append(jnp.sum(chosen, axis=0, keepdims=True))
    rows = jnp.concatenate(rows)
    row = lax.broadcasted_iota(jnp.int32, (count, count), 0)
    col = lax.broadcasted_iota(jnp.int32, (count, count), 1)
    columns = lax.dot_general(
        jnp.where(row == col, 1.0, 0.0),
        rows,
        (((1,), (1,)), ((), ())),
        precision=lax.Precision.HIGHEST,
        preferred_element_type=F32,
    )
    for slot in range(rows.shape[0]):
        out_ref[slot * count : (slot + 1) * count, :] = columns[:, slot : slot + 1]


def token_shares(place, tables):
    slots, count = 2 * len(tables), tables[0].shape[-1]
    return pl.pallas_call(
        share_kernel,
        out_shape=jax.ShapeDtypeStruct((slots * count, 1), F32),
        in_specs=[pl.BlockSpec(memory_space=pltpu.SMEM)] + in_vmem(len(tables)),
        out_specs=in_vmem(1)[0],
        compiler_params=room(4),
        name="share",
    )(place, *tables)


def last_norm_kernel(parts, groups, arrange, normed_ref, scale_ref, *refs):
    outs, refs = refs[-parts:], refs[:-parts]
    each = len(refs) // groups
    sums = []
    for k in range(groups):
        own, *others = refs[k * each : (k + 1) * each]
        total = own[...]
        for other in others:
            total = total + other[...].astype(F32)
        sums.append(total)
    rows = [
        ALPHA * normed_ref[k].astype(F32) + part for k, part in enumerate(arrange(*sums))
    ]
    features = sum(r.shape[1] for r in rows)
    mean = sum(jnp.sum(r, axis=1, keepdims=True) for r in rows) / features
    square = sum(jnp.sum(r * r, axis=1, keepdims=True) for r in rows) / features
    scale = lax.rsqrt(square - mean * mean + EPS)
    for k, out_ref in enumerate(outs):
        part = (rows[k] - mean) * scale * scale_ref[k, 2:3, :] + scale_ref[k, 3:4, :]
        out_ref[...] = part.astype(BF16)


def last_norm(arrange, normed, scales, groups):
    parts, count, wide = normed.shape
    flat = [r for group in groups for r in group]
    return pl.pallas_call(
        functools.partial(last_norm_kernel, parts, len(groups), arrange),
        out_shape=tuple(jax.ShapeDtypeStruct((count, wide), BF16) for _ in range(parts)),
        in_specs=in_vmem(2 + len(flat)),
        out_specs=tuple(in_vmem(parts)),
        compiler_params=room(12),
        name="last",
    )(normed, scales, *flat)


def weight_parts(w_gate, w_up, w_down, tp, later_of):
    if tp != 4:
        gate, up, down = (exchange_all(w, "tp") for w in (w_gate, w_up, w_down))
        pairs = [list(pair) for pair in zip(gate, up)]
        return pairs, [[w] for w in down], lambda *parts: list(parts)
    gate1 = swap_with(w_gate, "tp", 1)
    up2 = swap_with(w_up, "tp", 2)
    top = w_gate.shape[0] // 4
    later_gate, later_up = later_of(w_gate), later_of(w_up)
    up1_top = swap_with(later_up[:top], "tp", 1)
    gate2_top = swap_with(later_gate[:top], "tp", 2)
    up1_low = swap_with(later_up[top:], "tp", 1)
    gate2_low = swap_with(later_gate[top:], "tp", 2)
    up3 = swap_with(up2, "tp", 1)
    gate3 = swap_with(gate1, "tp", 2)
    wide = w_down.shape[1] // 2
    w_late = later_of(w_down)
    left, right = w_late[:, :wide], w_late[:, wide:]
    down1_l = swap_with(left, "tp", 1)
    down2_r = swap_with(right, "tp", 2)
    down1_r = swap_with(right, "tp", 1)
    down2_l = swap_with(left, "tp", 2)
    down3_r = swap_with(down2_r, "tp", 1)
    down3_l = swap_with(down1_l, "tp", 2)
    near = staged(
        [([w_gate], [w_up]), ([gate1], [up1_top, up1_low]), ([gate2_top, gate2_low], [up2])]
    )
    first = [[w] for w in near] + [[gate3, up3]]
    down = [[w_down], [down1_l, down2_r], [down1_r, down2_l], [down3_l, down3_r]]

    def by_distance(own, early, late, last):
        one = jnp.concatenate([early[:, :wide], late[:, :wide]], axis=1)
        two = jnp.concatenate([late[:, wide:], early[:, wide:]], axis=1)
        return [own, one, two, last]

    return first, down, by_distance


def body(
    pool_in,
    doc_ids,
    pool_map,
    pool_scale,
    w_out,
    gate_logit,
    residual,
    first_gain,
    first_bias,
    routes,
    route_weight,
    w_gate,
    w_up,
    w_down,
    second_gain,
    second_bias,
):
    sp, tp = lax.axis_size("sp"), lax.axis_size("tp")
    i, j = lax.axis_index("sp"), lax.axis_index("tp")
    _, positions = pool_in.shape
    quarter = positions // tp

    place = jnp.stack([i, j])
    gains = jnp.pad(
        jnp.stack([first_gain, first_bias, second_gain, second_bias]), ((0, 4), (0, 0))
    )
    gains = exchange_all(gains, "tp")
    pooled = pooled_channels(pool_in, doc_ids, place)

    def later_of(weight):
        return lax.optimization_barrier((weight, pooled))[0]

    first_w, down_w, by_distance = weight_parts(
        w_gate[0], w_up[0], w_down[0], tp, later_of
    )
    pooled_rel = exchange_all(pooled, "tp")
    my_routes = lax.dynamic_slice_in_dim(routes, j * quarter, quarter, 0)
    my_weights = lax.dynamic_slice_in_dim(route_weight, j * quarter, quarter, 0)
    chosen = jnp.stack([my_routes.astype(F32).T, my_weights.T])
    chosen = jnp.stack([chosen, swap_with(chosen, "sp", 1)])
    chosen = [chosen] + [swap_with(chosen, "sp", 2 * k) for k in range(1, sp // 2)]
    share = token_shares(place, chosen)

    gathered = jnp.concatenate(in_order(pooled_rel, j))
    group_count = gathered.shape[0] // GROUP_W
    grouped = jnp.einsum(
        "gct,gcd->tgd",
        gathered.reshape(group_count, GROUP_W, positions),
        pool_map,
        preferred_element_type=F32,
    )
    mapped = (grouped.reshape(positions, group_count * GROUP_W) * pool_scale).astype(BF16)
    mixer_out = jnp.dot(mapped, w_out, preferred_element_type=F32) * jax.nn.sigmoid(
        gate_logit.astype(F32)
    )
    mixed = ALPHA * residual.astype(F32) + mixer_out

    sent = rows_to_send(place, mixed, tp)
    both = [sent[0]] + [swap_with(sent[k], "tp", k) for k in range(1, tp)]
    tokens, normed, scales = first_norm(place, both, gains)

    everyone = line_gather(tokens, "sp")
    inputs, first_hidden = hidden_units(everyone, first_w[0])
    hidden_rel = [first_hidden] + [
        hidden_units([inputs], first_w[k])[1] for k in range(1, tp)
    ]

    groups = []
    half_rows = (sp // 2) * quarter
    for k in range(len(down_w)):
        partial = weighted_outputs(place, share, hidden_rel, down_w[k])
        other = swap_with(partial[half_rows:], "sp", 1)
        joined = partial[:half_rows].astype(F32) + other.astype(F32)
        sent = joined.astype(BF16)
        got = [
            swap_with(sent[d * quarter : (d + 1) * quarter], "sp", 2 * d)
            for d in range(1, sp // 2)
        ]
        groups.append([joined[:quarter]] + got)
    out_rel = last_norm(by_distance, normed, scales, groups)
    home_rel = [out_rel[0]] + [swap_with(out_rel[k], "tp", k) for k in range(1, tp)]
    return jnp.concatenate(in_order(home_rel, j))


def solution(mesh):
    return jax.shard_map(
        body,
        mesh=mesh,
        in_specs=(
            P("tp", "sp"),
            P("sp"),
            P(),
            P(),
            P(None, "tp"),
            P("sp", "tp"),
            P("sp", "tp"),
            P("tp"),
            P("tp"),
            P("sp", None),
            P("sp", None),
            P("sp", None, "tp"),
            P("sp", None, "tp"),
            P("sp", None, "tp"),
            P("tp"),
            P("tp"),
        ),
        out_specs=P("sp", "tp"),
        check_vma=False,
    )
```

```python
import functools

import jax
import jax.numpy as jnp
from jax import lax
from jax.experimental import pallas as pl
from jax.experimental.pallas import tpu as pltpu
from jax.sharding import PartitionSpec as P


GROUP_W = 64
EPS = 1e-05
ALPHA = 8.0**0.25
HALO = 16
F32 = jnp.float32
BF16 = jnp.bfloat16


def swap_with(part, axis, bits):
    size = lax.axis_size(axis)
    return lax.ppermute(part, axis, [(i, i ^ bits) for i in range(size)])


def in_order(relative, index):
    stacked = jnp.stack(relative)
    return [
        lax.dynamic_index_in_dim(stacked, index ^ p, 0, keepdims=False)
        for p in range(len(relative))
    ]


def exchange(parts, axis, unit):
    got = {0: parts[0]}
    for k in range(len(parts) - 1, 0, -1):
        got[k] = swap_with(parts[k], axis, unit * k)
    return [got[k] for k in range(len(parts))]


def exchange_all(part, axis):
    return exchange([part] * lax.axis_size(axis), axis, 1)


def line_gather(part, axis):
    size = lax.axis_size(axis)
    mine = exchange([part] * (size // 2), axis, 2)
    return mine + [swap_with(m, axis, 1) for m in mine]


TABLE = HALO + 8


def table_kernel(x_ref, docs_ref, table_ref):
    channels, positions = x_ref.shape
    docs = docs_ref[...].astype(F32).reshape(1, positions)
    last_doc = docs[:, positions - 1 :]
    ending = jnp.where(docs == last_doc, 1.0, 0.0)
    length = jnp.sum(ending, axis=1, keepdims=True)
    row = lax.broadcasted_iota(jnp.int32, (TABLE, positions), 0)
    col = lax.broadcasted_iota(jnp.int32, (TABLE, positions), 1)
    pick = jnp.where(col == positions - HALO + row, 1.0, 0.0)
    pick = jnp.where(row == HALO, jnp.broadcast_to(ending, pick.shape), pick)
    got = lax.dot_general(
        pick.astype(BF16), x_ref[...], (((1,), (1,)), ((), ())), preferred_element_type=F32
    )
    row = lax.broadcasted_iota(jnp.int32, (TABLE, channels), 0)
    got = jnp.where(row == HALO + 1, last_doc, got)
    table_ref[...] = jnp.where(row == HALO + 2, length, got)


def starts_of(docs_ref, positions):
    docs = jnp.broadcast_to(docs_ref[...].reshape(1, positions), (8, positions))
    lane = lax.broadcasted_iota(jnp.int32, (8, positions), 1)
    opens = (docs != pltpu.roll(docs, 1, 1)) & (lane > 0)
    start = jnp.where(opens, lane, 0)
    step = 1
    while step < positions:
        moved = pltpu.roll(start, step, 1)
        start = jnp.maximum(start, jnp.where(lane >= step, moved, 0))
        step *= 2
    return start


def units_of(channels, j):
    unit = min(GROUP_W, channels)
    for u in range(channels // unit):
        group = (j * channels + u * unit) // GROUP_W
        yield slice(u * unit, (u + 1) * unit), group % 2 == 1, lax.shift_left(2, group // 2 % 4)


def local_kernel(place_ref, x_ref, docs_ref, sum_ref, start_ref):
    channels, positions = x_ref.shape
    start_ref[...] = starts_of(docs_ref, positions)
    s_at = lax.broadcasted_iota(jnp.int32, (positions, positions), 0)
    t_at = lax.broadcasted_iota(jnp.int32, (positions, positions), 1)
    for rows, whole_doc, window in units_of(channels, place_ref[1]):
        reach = jnp.where(whole_doc, positions, window)
        lower = jnp.maximum(start_ref[:1, :], t_at[:1, :] + 1 - reach)
        mask = (s_at >= lower) & (s_at <= t_at)
        sum_ref[rows, :] = jnp.dot(
            x_ref[rows, :], mask.astype(BF16), preferred_element_type=F32
        )


def pooled_kernel(place_ref, x_ref, docs_ref, start_ref, sum_ref, *rest):
    *table_refs, out_ref = rest
    channels, positions = x_ref.shape
    i, j = place_ref[0], place_ref[1]
    first_doc = docs_ref[...].astype(F32).reshape(1, positions)[:, :1]
    before = jnp.zeros((TABLE, channels), F32)
    carried = jnp.zeros((TABLE, channels), F32)
    near_ref, *far_refs = table_refs
    for k in range(1, 2 * len(table_refs)):
        table = near_ref[...] if k == 1 else far_refs[k // 2 - 1][k % 2]
        earlier = jnp.where((i ^ k) < i, 1.0, 0.0)
        previous = jnp.where((i ^ k) == i - 1, 1.0, 0.0)
        same = jnp.where(table[HALO + 1 : HALO + 2, :1] == first_doc, earlier, 0.0)
        carried = carried + same * table
        before = before + previous * table
    count = carried[HALO + 2 : HALO + 3, :1]
    t_at = lax.broadcasted_iota(jnp.int32, (1, positions), 1)
    start = start_ref[:1, :]
    in_first = jnp.where(start == 0, 1.0, 0.0)
    doc_count = (t_at + 1 - start).astype(F32) + in_first * count
    row = lax.broadcasted_iota(jnp.int32, (TABLE, channels), 0)
    carry_row = jnp.where(row == HALO, carried, 0.0)
    over_first = jnp.broadcast_to(in_first, (TABLE, positions))
    carry = lax.dot_general(
        carry_row,
        over_first,
        (((0,), (0,)), ((), ())),
        precision=lax.Precision.HIGHEST,
        preferred_element_type=F32,
    )
    h_at = lax.broadcasted_iota(jnp.int32, (TABLE, positions), 0) - HALO
    reached = jnp.where(h_at.astype(F32) >= -count, over_first, 0.0)
    reached = jnp.where(h_at < 0, reached, 0.0)
    for rows, whole_doc, window in units_of(channels, j):
        halo_mask = jnp.where(h_at >= t_at + 1 - window, reached, 0.0)
        halo = lax.dot_general(
            before.astype(BF16),
            halo_mask.astype(BF16),
            (((0,), (0,)), ((), ())),
            preferred_element_type=F32,
        )
        whole = jnp.where(whole_doc, 1.0, 0.0)
        total = sum_ref[rows, :] + whole * carry[rows] + (1.0 - whole) * halo[rows]
        most = jnp.where(whole_doc, float(1 << 30), window.astype(F32))
        total = total / jnp.minimum(doc_count, most)
        out_ref[rows, :] = (total - x_ref[rows, :].astype(F32)).astype(BF16)


def in_vmem(count):
    return [pl.BlockSpec(memory_space=pltpu.VMEM)] * count


def room(mebibytes):
    return pltpu.CompilerParams(vmem_limit_bytes=mebibytes << 20)


def table_call(pool_in, doc_ids):
    return pl.pallas_call(
        table_kernel,
        out_shape=jax.ShapeDtypeStruct((TABLE, pool_in.shape[0]), F32),
        in_specs=in_vmem(2),
        out_specs=in_vmem(1)[0],
        compiler_params=room(4),
        name="table",
    )(pool_in, doc_ids)


def pooled_channels(pool_in, doc_ids, place):
    channels, positions = pool_in.shape
    scalars = pl.BlockSpec(memory_space=pltpu.SMEM)
    table = table_call(pool_in, doc_ids)
    near = swap_with(table, "sp", 1)
    pair = jnp.stack([table, near])
    sums, start = pl.pallas_call(
        local_kernel,
        out_shape=(
            jax.ShapeDtypeStruct((channels, positions), F32),
            jax.ShapeDtypeStruct((8, positions), jnp.int32),
        ),
        in_specs=[scalars] + in_vmem(2),
        out_specs=tuple(in_vmem(2)),
        compiler_params=room(8),
        name="local",
    )(place, pool_in, doc_ids)
    far = [swap_with(pair, "sp", 2 * k) for k in range(1, lax.axis_size("sp") // 2)]
    return pl.pallas_call(
        pooled_kernel,
        out_shape=jax.ShapeDtypeStruct((channels, positions), BF16),
        in_specs=[scalars] + in_vmem(5 + len(far)),
        out_specs=in_vmem(1)[0],
        compiler_params=room(8),
        name="pooled",
    )(place, pool_in, doc_ids, start, sums, near, *far)


def gather_rows_kernel(*refs):
    *parts, out_ref = refs
    rows = parts[0].shape[0]
    for p, part in enumerate(parts):
        out_ref[p * rows : (p + 1) * rows, :] = part[...]


def hidden_kernel(count, *refs):
    row_refs, weights, outs = refs[:count], refs[count:-1], refs[-1:]
    if count > 1:
        weights, outs = refs[count:-2], refs[-2:]
        gather_rows_kernel(*row_refs, outs[0])
    rows = outs[0] if count > 1 else row_refs[0]
    if len(weights) == 1:
        both = jnp.dot(rows[...], weights[0][...], preferred_element_type=F32)
        half = both.shape[1] // 2
        gated, up = both[:, :half], both[:, half:]
    else:
        gated, up = (
            jnp.dot(rows[...], w[...], preferred_element_type=F32) for w in weights
        )
    outs[-1][...] = (gated * jax.nn.sigmoid(gated) * up).astype(BF16)


def hidden_units(row_parts, weights):
    count = len(row_parts)
    rows = sum(r.shape[0] for r in row_parts)
    wide = sum(w.shape[1] for w in weights) // 2
    shape = jax.ShapeDtypeStruct((rows, wide), BF16)
    joined = jax.ShapeDtypeStruct((rows, row_parts[0].shape[1]), BF16)
    outs = (joined, shape) if count > 1 else (shape,)
    got = pl.pallas_call(
        functools.partial(hidden_kernel, count),
        out_shape=outs,
        in_specs=in_vmem(count + len(weights)),
        out_specs=tuple(in_vmem(len(outs))),
        compiler_params=room(20),
        name="hidden",
    )(*row_parts, *weights)
    return (got[0], got[-1])


def stage_kernel(pieces, *refs):
    at = 0
    outs = refs[sum(sum(p) for p in pieces) :]
    for out, pair in zip(outs, pieces):
        half = out.shape[1] // 2
        for side, count in enumerate(pair):
            row = 0
            for ref in refs[at : at + count]:
                depth = ref.shape[0]
                out[row : row + depth, side * half : (side + 1) * half] = ref[...]
                row += depth
            at += count


def staged(pairs):
    flat = [w for pair in pairs for side in pair for w in side]
    pieces = tuple(tuple(len(side) for side in pair) for pair in pairs)
    depth = sum(w.shape[0] for w in pairs[0][0])
    return pl.pallas_call(
        functools.partial(stage_kernel, pieces),
        out_shape=tuple(
            jax.ShapeDtypeStruct((depth, 2 * pair[0][0].shape[1]), BF16) for pair in pairs
        ),
        in_specs=in_vmem(len(flat)),
        out_specs=tuple(in_vmem(len(pairs))),
        compiler_params=room(16),
        name="stage",
    )(*flat)


def down_kernel(parts, first, place_ref, share_ref, *refs):
    hidden, weights, out_ref = refs[:parts], refs[parts:-1], refs[-1]
    depth, total = hidden[0].shape[1], None
    kept = slice(first, first + out_ref.shape[0])
    for k in range(parts):
        rows = pl.ds(pl.multiple_of((place_ref[1] ^ k) * depth, depth), depth)
        near = [weight[rows, :] for weight in weights]
        near = near[0] if len(near) == 1 else jnp.concatenate(near, axis=1)
        piece = jnp.dot(hidden[k][kept, :], near, preferred_element_type=F32)
        total = piece if total is None else total + piece
    out_ref[...] = (total * share_ref[kept, :]).astype(out_ref.dtype)


def weighted_outputs(place, share, hidden, weights, first, rows, dtype):
    wide = sum(w.shape[1] for w in weights)
    return pl.pallas_call(
        functools.partial(down_kernel, len(hidden), first),
        out_shape=jax.ShapeDtypeStruct((rows, wide), dtype),
        in_specs=[pl.BlockSpec(memory_space=pltpu.SMEM)]
        + in_vmem(1 + len(hidden) + len(weights)),
        out_specs=in_vmem(1)[0],
        compiler_params=room(14),
        name="down",
    )(place, share, *hidden, *weights)


LANES = 128


def rows_kernel(place_ref, mixed_ref, *outs):
    count, wide = outs[0].shape[0], mixed_ref.shape[1]
    lane = lax.broadcasted_iota(jnp.int32, (count, LANES), 1)
    for k, out_ref in enumerate(outs):
        at = pl.multiple_of((place_ref[1] ^ k) * count, 8)
        part = mixed_ref[pl.ds(at, count), :]
        mean = jnp.sum(part, axis=1, keepdims=True) / wide
        out_ref[:, :wide] = (part - mean).astype(BF16)
        high = mean.astype(BF16).astype(F32)
        middle = (mean - high).astype(BF16).astype(F32)
        low = mean - high - middle
        terms = jnp.where(lane == 0, high, jnp.where(lane == 1, middle, low))
        out_ref[:, wide:] = terms.astype(BF16)


def rows_to_send(place, mixed, parts):
    count, wide = mixed.shape[0] // parts, mixed.shape[1]
    return pl.pallas_call(
        rows_kernel,
        out_shape=tuple(
            jax.ShapeDtypeStruct((count, wide + LANES), BF16) for _ in range(parts)
        ),
        in_specs=[pl.BlockSpec(memory_space=pltpu.SMEM)] + in_vmem(1),
        out_specs=tuple(in_vmem(parts)),
        compiler_params=room(4),
        name="rows",
    )(place, mixed)


def first_norm_kernel(parts, place_ref, *refs):
    rows, gains, outs = refs[:parts], refs[parts : 2 * parts], refs[2 * parts :]
    tokens_ref, normed_ref, scale_ref = outs
    wide = normed_ref.shape[2]
    values = []
    for ref in rows:
        mean = ref[:, wide : wide + 3].astype(F32)
        mean = mean[:, :1] + mean[:, 1:2] + mean[:, 2:3]
        values.append(ref[:, :wide].astype(F32) + mean)
    features = parts * wide
    mean = sum(jnp.sum(v, axis=1, keepdims=True) for v in values) / features
    square = sum(jnp.sum(v * v, axis=1, keepdims=True) for v in values) / features
    scale = lax.rsqrt(square - mean * mean + EPS)
    for k, value in enumerate(values):
        scale_ref[k] = gains[k][...]
        part = (value - mean) * scale * gains[k][:1, :] + gains[k][1:2, :]
        part = part.astype(BF16)
        normed_ref[k] = part
        at = pl.multiple_of((place_ref[1] ^ k) * wide, wide)
        tokens_ref[:, pl.ds(at, wide)] = part


def first_norm(place, rows, gains):
    parts, count = len(rows), rows[0].shape[0]
    wide = gains[0].shape[1]
    return pl.pallas_call(
        functools.partial(first_norm_kernel, parts),
        out_shape=(
            jax.ShapeDtypeStruct((count, parts * wide), BF16),
            jax.ShapeDtypeStruct((parts, count, wide), BF16),
            jax.ShapeDtypeStruct((parts,) + gains[0].shape, F32),
        ),
        in_specs=[pl.BlockSpec(memory_space=pltpu.SMEM)] + in_vmem(2 * parts),
        out_specs=tuple(in_vmem(3)),
        compiler_params=room(8),
        name="norm",
    )(place, *rows, *gains)


def share_kernel(place_ref, *refs):
    *tables, out_ref = refs
    count = tables[0].shape[-1]
    mine = place_ref[0].astype(F32)
    rows = []
    for core in range(2):
        for table in tables:
            chosen = jnp.where(table[core, 0] == mine, table[core, 1], 0.0)
            rows.append(jnp.sum(chosen, axis=0, keepdims=True))
    rows = jnp.concatenate(rows)
    row = lax.broadcasted_iota(jnp.int32, (count, count), 0)
    col = lax.broadcasted_iota(jnp.int32, (count, count), 1)
    columns = lax.dot_general(
        jnp.where(row == col, 1.0, 0.0),
        rows,
        (((1,), (1,)), ((), ())),
        precision=lax.Precision.HIGHEST,
        preferred_element_type=F32,
    )
    for slot in range(rows.shape[0]):
        out_ref[slot * count : (slot + 1) * count, :] = columns[:, slot : slot + 1]


def token_shares(place, tables):
    slots, count = 2 * len(tables), tables[0].shape[-1]
    return pl.pallas_call(
        share_kernel,
        out_shape=jax.ShapeDtypeStruct((slots * count, 1), F32),
        in_specs=[pl.BlockSpec(memory_space=pltpu.SMEM)] + in_vmem(len(tables)),
        out_specs=in_vmem(1)[0],
        compiler_params=room(4),
        name="share",
    )(place, *tables)


def last_norm_kernel(parts, groups, arrange, normed_ref, scale_ref, *refs):
    outs, refs = refs[-parts:], refs[:-parts]
    each = len(refs) // groups
    sums = []
    for k in range(groups):
        own, *others = refs[k * each : (k + 1) * each]
        total = own[...]
        for other in others:
            total = total + other[...].astype(F32)
        sums.append(total)
    rows = [
        ALPHA * normed_ref[k].astype(F32) + part for k, part in enumerate(arrange(*sums))
    ]
    features = sum(r.shape[1] for r in rows)
    mean = sum(jnp.sum(r, axis=1, keepdims=True) for r in rows) / features
    square = sum(jnp.sum(r * r, axis=1, keepdims=True) for r in rows) / features
    scale = lax.rsqrt(square - mean * mean + EPS)
    for k, out_ref in enumerate(outs):
        part = (rows[k] - mean) * scale * scale_ref[k, 2:3, :] + scale_ref[k, 3:4, :]
        out_ref[...] = part.astype(BF16)


def last_norm(arrange, normed, scales, groups):
    parts, count, wide = normed.shape
    flat = [r for group in groups for r in group]
    return pl.pallas_call(
        functools.partial(last_norm_kernel, parts, len(groups), arrange),
        out_shape=tuple(jax.ShapeDtypeStruct((count, wide), BF16) for _ in range(parts)),
        in_specs=in_vmem(2 + len(flat)),
        out_specs=tuple(in_vmem(parts)),
        compiler_params=room(12),
        name="last",
    )(normed, scales, *flat)


def weight_parts(w_gate, w_up, w_down, tp, later_of):
    if tp != 4:
        gate, up, down = (exchange_all(w, "tp") for w in (w_gate, w_up, w_down))
        pairs = [list(pair) for pair in zip(gate, up)]
        return pairs, [[w] for w in down], lambda *parts: list(parts)
    gate1 = swap_with(w_gate, "tp", 1)
    up2 = swap_with(w_up, "tp", 2)
    top = w_gate.shape[0] * 5 // 16
    later_gate, later_up = later_of(w_gate), later_of(w_up)
    up1_top = swap_with(later_up[:top], "tp", 1)
    gate2_top = swap_with(later_gate[:top], "tp", 2)
    up1_low = swap_with(later_up[top:], "tp", 1)
    gate2_low = swap_with(later_gate[top:], "tp", 2)
    up3 = swap_with(up2, "tp", 1)
    gate3 = swap_with(gate1, "tp", 2)
    wide = w_down.shape[1] // 2
    w_late = later_of(w_down)
    left, right = w_late[:, :wide], w_late[:, wide:]
    down1_l = swap_with(left, "tp", 1)
    down2_r = swap_with(right, "tp", 2)
    down1_r = swap_with(right, "tp", 1)
    down2_l = swap_with(left, "tp", 2)
    down3_r = swap_with(down2_r, "tp", 1)
    down3_l = swap_with(down1_l, "tp", 2)
    near = staged(
        [([w_gate], [w_up]), ([gate1], [up1_top, up1_low]), ([gate2_top, gate2_low], [up2])]
    )
    first = [[w] for w in near] + [[gate3, up3]]
    down = [[w_down], [down1_l, down2_r], [down1_r, down2_l], [down3_l, down3_r]]

    def by_distance(own, early, late, last):
        one = jnp.concatenate([early[:, :wide], late[:, :wide]], axis=1)
        two = jnp.concatenate([late[:, wide:], early[:, wide:]], axis=1)
        return [own, one, two, last]

    return first, down, by_distance


def body(
    pool_in,
    doc_ids,
    pool_map,
    pool_scale,
    w_out,
    gate_logit,
    residual,
    first_gain,
    first_bias,
    routes,
    route_weight,
    w_gate,
    w_up,
    w_down,
    second_gain,
    second_bias,
):
    sp, tp = lax.axis_size("sp"), lax.axis_size("tp")
    i, j = lax.axis_index("sp"), lax.axis_index("tp")
    _, positions = pool_in.shape
    quarter = positions // tp

    place = jnp.stack([i, j])
    gains = jnp.pad(
        jnp.stack([first_gain, first_bias, second_gain, second_bias]), ((0, 4), (0, 0))
    )
    gains = exchange_all(gains, "tp")
    pooled = pooled_channels(pool_in, doc_ids, place)

    def later_of(weight):
        return lax.optimization_barrier((weight, pooled))[0]

    first_w, down_w, by_distance = weight_parts(
        w_gate[0], w_up[0], w_down[0], tp, later_of
    )
    pooled_rel = exchange_all(pooled, "tp")
    my_routes = lax.dynamic_slice_in_dim(routes, j * quarter, quarter, 0)
    my_weights = lax.dynamic_slice_in_dim(route_weight, j * quarter, quarter, 0)
    chosen = jnp.stack([my_routes.astype(F32).T, my_weights.T])
    chosen = jnp.stack([chosen, swap_with(chosen, "sp", 1)])
    chosen = [chosen] + [swap_with(chosen, "sp", 2 * k) for k in range(1, sp // 2)]
    share = token_shares(place, chosen)

    gathered = jnp.concatenate(in_order(pooled_rel, j))
    group_count = gathered.shape[0] // GROUP_W
    grouped = jnp.einsum(
        "gct,gcd->tgd",
        gathered.reshape(group_count, GROUP_W, positions),
        pool_map,
        preferred_element_type=F32,
    )
    mapped = (grouped.reshape(positions, group_count * GROUP_W) * pool_scale).astype(BF16)
    mixer_out = jnp.dot(mapped, w_out, preferred_element_type=F32) * jax.nn.sigmoid(
        gate_logit.astype(F32)
    )
    mixed = ALPHA * residual.astype(F32) + mixer_out

    sent = rows_to_send(place, mixed, tp)
    both = exchange(sent, "tp", 1)
    tokens, normed, scales = first_norm(place, both, gains)

    everyone = line_gather(tokens, "sp")
    inputs, first_hidden = hidden_units(everyone, first_w[0])
    hidden_rel = [first_hidden] + [
        hidden_units([inputs], first_w[k])[1] for k in range(1, tp)
    ]

    groups = []
    half_rows = (sp // 2) * quarter
    for k in range(len(down_w)):
        common = (place, share, hidden_rel, down_w[k])
        other = weighted_outputs(*common, half_rows, half_rows, BF16)
        other = swap_with(other, "sp", 1)
        own = weighted_outputs(*common, 0, half_rows, F32)
        joined = own + other.astype(F32)
        sent = joined.astype(BF16)
        got = exchange(
            [sent[d * quarter : (d + 1) * quarter] for d in range(sp // 2)], "sp", 2
        )
        groups.append([joined[:quarter]] + got[1:])
    out_rel = last_norm(by_distance, normed, scales, groups)
    home_rel = exchange(out_rel, "tp", 1)
    return jnp.concatenate(in_order(home_rel, j))


def solution(mesh):
    return jax.shard_map(
        body,
        mesh=mesh,
        in_specs=(
            P("tp", "sp"),
            P("sp"),
            P(),
            P(),
            P(None, "tp"),
            P("sp", "tp"),
            P("sp", "tp"),
            P("tp"),
            P("tp"),
            P("sp", None),
            P("sp", None),
            P("sp", None, "tp"),
            P("sp", None, "tp"),
            P("sp", None, "tp"),
            P("tp"),
            P("tp"),
        ),
        out_specs=P("sp", "tp"),
        check_vma=False,
    )
```

```python
import functools

import jax
import jax.numpy as jnp
from jax import lax
from jax.experimental import pallas as pl
from jax.experimental.pallas import tpu as pltpu
from jax.sharding import PartitionSpec as P


GROUP_W = 64
EPS = 1e-05
ALPHA = 8.0**0.25
HALO = 16
F32 = jnp.float32
BF16 = jnp.bfloat16


def swap_with(part, axis, bits):
    size = lax.axis_size(axis)
    return lax.ppermute(part, axis, [(i, i ^ bits) for i in range(size)])


def in_order(relative, index):
    stacked = jnp.stack(relative)
    return [
        lax.dynamic_index_in_dim(stacked, index ^ p, 0, keepdims=False)
        for p in range(len(relative))
    ]


def exchange(parts, axis, unit):
    got = {0: parts[0]}
    for k in range(len(parts) - 1, 0, -1):
        got[k] = swap_with(parts[k], axis, unit * k)
    return [got[k] for k in range(len(parts))]


def exchange_all(part, axis):
    return exchange([part] * lax.axis_size(axis), axis, 1)


def line_gather(part, axis):
    size = lax.axis_size(axis)
    mine = exchange([part] * (size // 2), axis, 2)
    return mine + [swap_with(m, axis, 1) for m in mine]


TABLE = HALO + 8


def table_kernel(x_ref, docs_ref, table_ref):
    channels, positions = x_ref.shape
    docs = docs_ref[...].astype(F32).reshape(1, positions)
    last_doc = docs[:, positions - 1 :]
    ending = jnp.where(docs == last_doc, 1.0, 0.0)
    length = jnp.sum(ending, axis=1, keepdims=True)
    row = lax.broadcasted_iota(jnp.int32, (TABLE, positions), 0)
    col = lax.broadcasted_iota(jnp.int32, (TABLE, positions), 1)
    pick = jnp.where(col == positions - HALO + row, 1.0, 0.0)
    pick = jnp.where(row == HALO, jnp.broadcast_to(ending, pick.shape), pick)
    got = lax.dot_general(
        pick.astype(BF16), x_ref[...], (((1,), (1,)), ((), ())), preferred_element_type=F32
    )
    row = lax.broadcasted_iota(jnp.int32, (TABLE, channels), 0)
    got = jnp.where(row == HALO + 1, last_doc, got)
    table_ref[...] = jnp.where(row == HALO + 2, length, got)


def starts_of(docs_ref, positions):
    docs = jnp.broadcast_to(docs_ref[...].reshape(1, positions), (8, positions))
    lane = lax.broadcasted_iota(jnp.int32, (8, positions), 1)
    opens = (docs != pltpu.roll(docs, 1, 1)) & (lane > 0)
    start = jnp.where(opens, lane, 0)
    step = 1
    while step < positions:
        moved = pltpu.roll(start, step, 1)
        start = jnp.maximum(start, jnp.where(lane >= step, moved, 0))
        step *= 2
    return start


def units_of(channels, j):
    unit = min(GROUP_W, channels)
    for u in range(channels // unit):
        group = (j * channels + u * unit) // GROUP_W
        yield slice(u * unit, (u + 1) * unit), group % 2 == 1, lax.shift_left(2, group // 2 % 4)


def local_kernel(place_ref, x_ref, docs_ref, sum_ref, start_ref):
    channels, positions = x_ref.shape
    start_ref[...] = starts_of(docs_ref, positions)
    s_at = lax.broadcasted_iota(jnp.int32, (positions, positions), 0)
    t_at = lax.broadcasted_iota(jnp.int32, (positions, positions), 1)
    for rows, whole_doc, window in units_of(channels, place_ref[1]):
        reach = jnp.where(whole_doc, positions, window)
        lower = jnp.maximum(start_ref[:1, :], t_at[:1, :] + 1 - reach)
        mask = (s_at >= lower) & (s_at <= t_at)
        sum_ref[rows, :] = jnp.dot(
            x_ref[rows, :], mask.astype(BF16), preferred_element_type=F32
        )


def pooled_kernel(place_ref, x_ref, docs_ref, start_ref, sum_ref, *rest):
    *table_refs, out_ref = rest
    channels, positions = x_ref.shape
    i, j = place_ref[0], place_ref[1]
    first_doc = docs_ref[...].astype(F32).reshape(1, positions)[:, :1]
    before = jnp.zeros((TABLE, channels), F32)
    carried = jnp.zeros((TABLE, channels), F32)
    near_ref, *far_refs = table_refs
    for k in range(1, 2 * len(table_refs)):
        table = near_ref[...] if k == 1 else far_refs[k // 2 - 1][k % 2]
        earlier = jnp.where((i ^ k) < i, 1.0, 0.0)
        previous = jnp.where((i ^ k) == i - 1, 1.0, 0.0)
        same = jnp.where(table[HALO + 1 : HALO + 2, :1] == first_doc, earlier, 0.0)
        carried = carried + same * table
        before = before + previous * table
    count = carried[HALO + 2 : HALO + 3, :1]
    t_at = lax.broadcasted_iota(jnp.int32, (1, positions), 1)
    start = start_ref[:1, :]
    in_first = jnp.where(start == 0, 1.0, 0.0)
    doc_count = (t_at + 1 - start).astype(F32) + in_first * count
    row = lax.broadcasted_iota(jnp.int32, (TABLE, channels), 0)
    carry_row = jnp.where(row == HALO, carried, 0.0)
    over_first = jnp.broadcast_to(in_first, (TABLE, positions))
    carry = lax.dot_general(
        carry_row,
        over_first,
        (((0,), (0,)), ((), ())),
        precision=lax.Precision.HIGHEST,
        preferred_element_type=F32,
    )
    h_at = lax.broadcasted_iota(jnp.int32, (TABLE, positions), 0) - HALO
    reached = jnp.where(h_at.astype(F32) >= -count, over_first, 0.0)
    reached = jnp.where(h_at < 0, reached, 0.0)
    for rows, whole_doc, window in units_of(channels, j):
        halo_mask = jnp.where(h_at >= t_at + 1 - window, reached, 0.0)
        halo = lax.dot_general(
            before.astype(BF16),
            halo_mask.astype(BF16),
            (((0,), (0,)), ((), ())),
            preferred_element_type=F32,
        )
        whole = jnp.where(whole_doc, 1.0, 0.0)
        total = sum_ref[rows, :] + whole * carry[rows] + (1.0 - whole) * halo[rows]
        most = jnp.where(whole_doc, float(1 << 30), window.astype(F32))
        total = total / jnp.minimum(doc_count, most)
        out_ref[rows, :] = (total - x_ref[rows, :].astype(F32)).astype(BF16)


def in_vmem(count):
    return [pl.BlockSpec(memory_space=pltpu.VMEM)] * count


def room(mebibytes):
    return pltpu.CompilerParams(vmem_limit_bytes=mebibytes << 20)


def table_call(pool_in, doc_ids):
    return pl.pallas_call(
        table_kernel,
        out_shape=jax.ShapeDtypeStruct((TABLE, pool_in.shape[0]), F32),
        in_specs=in_vmem(2),
        out_specs=in_vmem(1)[0],
        compiler_params=room(4),
        name="table",
    )(pool_in, doc_ids)


def pooled_channels(pool_in, doc_ids, place):
    channels, positions = pool_in.shape
    scalars = pl.BlockSpec(memory_space=pltpu.SMEM)
    table = table_call(pool_in, doc_ids)
    near = swap_with(table, "sp", 1)
    pair = jnp.stack([table, near])
    sums, start = pl.pallas_call(
        local_kernel,
        out_shape=(
            jax.ShapeDtypeStruct((channels, positions), F32),
            jax.ShapeDtypeStruct((8, positions), jnp.int32),
        ),
        in_specs=[scalars] + in_vmem(2),
        out_specs=tuple(in_vmem(2)),
        compiler_params=room(8),
        name="local",
    )(place, pool_in, doc_ids)
    far = [swap_with(pair, "sp", 2 * k) for k in range(1, lax.axis_size("sp") // 2)]
    return pl.pallas_call(
        pooled_kernel,
        out_shape=jax.ShapeDtypeStruct((channels, positions), BF16),
        in_specs=[scalars] + in_vmem(5 + len(far)),
        out_specs=in_vmem(1)[0],
        compiler_params=room(8),
        name="pooled",
    )(place, pool_in, doc_ids, start, sums, near, *far)


def gather_rows_kernel(*refs):
    *parts, out_ref = refs
    rows = parts[0].shape[0]
    for p, part in enumerate(parts):
        out_ref[p * rows : (p + 1) * rows, :] = part[...]


def hidden_kernel(count, *refs):
    row_refs, weights, outs = refs[:count], refs[count:-1], refs[-1:]
    if count > 1:
        weights, outs = refs[count:-2], refs[-2:]
        gather_rows_kernel(*row_refs, outs[0])
    rows = outs[0] if count > 1 else row_refs[0]
    if len(weights) == 1:
        both = jnp.dot(rows[...], weights[0][...], preferred_element_type=F32)
        half = both.shape[1] // 2
        gated, up = both[:, :half], both[:, half:]
    else:
        gated, up = (
            jnp.dot(rows[...], w[...], preferred_element_type=F32) for w in weights
        )
    outs[-1][...] = (gated * jax.nn.sigmoid(gated) * up).astype(BF16)


def hidden_units(row_parts, weights):
    count = len(row_parts)
    rows = sum(r.shape[0] for r in row_parts)
    wide = sum(w.shape[1] for w in weights) // 2
    shape = jax.ShapeDtypeStruct((rows, wide), BF16)
    joined = jax.ShapeDtypeStruct((rows, row_parts[0].shape[1]), BF16)
    outs = (joined, shape) if count > 1 else (shape,)
    got = pl.pallas_call(
        functools.partial(hidden_kernel, count),
        out_shape=outs,
        in_specs=in_vmem(count + len(weights)),
        out_specs=tuple(in_vmem(len(outs))),
        compiler_params=room(20),
        name="hidden",
    )(*row_parts, *weights)
    return (got[0], got[-1])


def stage_kernel(pieces, *refs):
    at = 0
    outs = refs[sum(sum(p) for p in pieces) :]
    for out, pair in zip(outs, pieces):
        half = out.shape[1] // 2
        for side, count in enumerate(pair):
            row = 0
            for ref in refs[at : at + count]:
                depth = ref.shape[0]
                out[row : row + depth, side * half : (side + 1) * half] = ref[...]
                row += depth
            at += count


def staged(pairs):
    flat = [w for pair in pairs for side in pair for w in side]
    pieces = tuple(tuple(len(side) for side in pair) for pair in pairs)
    depth = sum(w.shape[0] for w in pairs[0][0])
    return pl.pallas_call(
        functools.partial(stage_kernel, pieces),
        out_shape=tuple(
            jax.ShapeDtypeStruct((depth, 2 * pair[0][0].shape[1]), BF16) for pair in pairs
        ),
        in_specs=in_vmem(len(flat)),
        out_specs=tuple(in_vmem(len(pairs))),
        compiler_params=room(16),
        name="stage",
    )(*flat)


def down_kernel(parts, first, place_ref, share_ref, *refs):
    hidden, weights, out_ref = refs[:parts], refs[parts:-1], refs[-1]
    depth, total = hidden[0].shape[1], None
    kept = slice(first, first + out_ref.shape[0])
    for k in range(parts):
        rows = pl.ds(pl.multiple_of((place_ref[1] ^ k) * depth, depth), depth)
        near = [weight[rows, :] for weight in weights]
        near = near[0] if len(near) == 1 else jnp.concatenate(near, axis=1)
        piece = jnp.dot(hidden[k][kept, :], near, preferred_element_type=F32)
        total = piece if total is None else total + piece
    out_ref[...] = (total * share_ref[kept, :]).astype(out_ref.dtype)


def weighted_outputs(place, share, hidden, weights, first, rows, dtype):
    wide = sum(w.shape[1] for w in weights)
    return pl.pallas_call(
        functools.partial(down_kernel, len(hidden), first),
        out_shape=jax.ShapeDtypeStruct((rows, wide), dtype),
        in_specs=[pl.BlockSpec(memory_space=pltpu.SMEM)]
        + in_vmem(1 + len(hidden) + len(weights)),
        out_specs=in_vmem(1)[0],
        compiler_params=room(14),
        name="down",
    )(place, share, *hidden, *weights)


LANES = 128


def rows_kernel(place_ref, mixed_ref, *outs):
    count, wide = outs[0].shape[0], mixed_ref.shape[1]
    lane = lax.broadcasted_iota(jnp.int32, (count, LANES), 1)
    for k, out_ref in enumerate(outs):
        at = pl.multiple_of((place_ref[1] ^ k) * count, 8)
        part = mixed_ref[pl.ds(at, count), :]
        mean = jnp.sum(part, axis=1, keepdims=True) / wide
        out_ref[:, :wide] = (part - mean).astype(BF16)
        high = mean.astype(BF16).astype(F32)
        middle = (mean - high).astype(BF16).astype(F32)
        low = mean - high - middle
        terms = jnp.where(lane == 0, high, jnp.where(lane == 1, middle, low))
        out_ref[:, wide:] = terms.astype(BF16)


def rows_to_send(place, mixed, parts):
    count, wide = mixed.shape[0] // parts, mixed.shape[1]
    return pl.pallas_call(
        rows_kernel,
        out_shape=tuple(
            jax.ShapeDtypeStruct((count, wide + LANES), BF16) for _ in range(parts)
        ),
        in_specs=[pl.BlockSpec(memory_space=pltpu.SMEM)] + in_vmem(1),
        out_specs=tuple(in_vmem(parts)),
        compiler_params=room(4),
        name="rows",
    )(place, mixed)


def first_norm_kernel(parts, place_ref, *refs):
    rows, gains, outs = refs[:parts], refs[parts : 2 * parts], refs[2 * parts :]
    tokens_ref, normed_ref, scale_ref = outs
    wide = normed_ref.shape[2]
    values = []
    for ref in rows:
        mean = ref[:, wide : wide + 3].astype(F32)
        mean = mean[:, :1] + mean[:, 1:2] + mean[:, 2:3]
        values.append(ref[:, :wide].astype(F32) + mean)
    features = parts * wide
    mean = sum(jnp.sum(v, axis=1, keepdims=True) for v in values) / features
    square = sum(jnp.sum(v * v, axis=1, keepdims=True) for v in values) / features
    scale = lax.rsqrt(square - mean * mean + EPS)
    for k, value in enumerate(values):
        scale_ref[k] = gains[k][...]
        part = (value - mean) * scale * gains[k][:1, :] + gains[k][1:2, :]
        part = part.astype(BF16)
        normed_ref[k] = part
        at = pl.multiple_of((place_ref[1] ^ k) * wide, wide)
        tokens_ref[:, pl.ds(at, wide)] = part


def first_norm(place, rows, gains):
    parts, count = len(rows), rows[0].shape[0]
    wide = gains[0].shape[1]
    return pl.pallas_call(
        functools.partial(first_norm_kernel, parts),
        out_shape=(
            jax.ShapeDtypeStruct((count, parts * wide), BF16),
            jax.ShapeDtypeStruct((parts, count, wide), BF16),
            jax.ShapeDtypeStruct((parts,) + gains[0].shape, F32),
        ),
        in_specs=[pl.BlockSpec(memory_space=pltpu.SMEM)] + in_vmem(2 * parts),
        out_specs=tuple(in_vmem(3)),
        compiler_params=room(8),
        name="norm",
    )(place, *rows, *gains)


def share_kernel(place_ref, *refs):
    *tables, out_ref = refs
    count = tables[0].shape[-1]
    mine = place_ref[0].astype(F32)
    rows = []
    for core in range(2):
        for table in tables:
            chosen = jnp.where(table[core, 0] == mine, table[core, 1], 0.0)
            rows.append(jnp.sum(chosen, axis=0, keepdims=True))
    rows = jnp.concatenate(rows)
    row = lax.broadcasted_iota(jnp.int32, (count, count), 0)
    col = lax.broadcasted_iota(jnp.int32, (count, count), 1)
    columns = lax.dot_general(
        jnp.where(row == col, 1.0, 0.0),
        rows,
        (((1,), (1,)), ((), ())),
        precision=lax.Precision.HIGHEST,
        preferred_element_type=F32,
    )
    for slot in range(rows.shape[0]):
        out_ref[slot * count : (slot + 1) * count, :] = columns[:, slot : slot + 1]


def token_shares(place, tables):
    slots, count = 2 * len(tables), tables[0].shape[-1]
    return pl.pallas_call(
        share_kernel,
        out_shape=jax.ShapeDtypeStruct((slots * count, 1), F32),
        in_specs=[pl.BlockSpec(memory_space=pltpu.SMEM)] + in_vmem(len(tables)),
        out_specs=in_vmem(1)[0],
        compiler_params=room(4),
        name="share",
    )(place, *tables)


def last_norm_kernel(parts, groups, arrange, normed_ref, scale_ref, *refs):
    outs, refs = refs[-parts:], refs[:-parts]
    each = len(refs) // groups
    sums = []
    for k in range(groups):
        own, *others = refs[k * each : (k + 1) * each]
        total = own[...]
        for other in others:
            total = total + other[...].astype(F32)
        sums.append(total)
    rows = [
        ALPHA * normed_ref[k].astype(F32) + part for k, part in enumerate(arrange(*sums))
    ]
    features = sum(r.shape[1] for r in rows)
    mean = sum(jnp.sum(r, axis=1, keepdims=True) for r in rows) / features
    square = sum(jnp.sum(r * r, axis=1, keepdims=True) for r in rows) / features
    scale = lax.rsqrt(square - mean * mean + EPS)
    for k, out_ref in enumerate(outs):
        part = (rows[k] - mean) * scale * scale_ref[k, 2:3, :] + scale_ref[k, 3:4, :]
        out_ref[...] = part.astype(BF16)


def last_norm(arrange, normed, scales, groups):
    parts, count, wide = normed.shape
    flat = [r for group in groups for r in group]
    return pl.pallas_call(
        functools.partial(last_norm_kernel, parts, len(groups), arrange),
        out_shape=tuple(jax.ShapeDtypeStruct((count, wide), BF16) for _ in range(parts)),
        in_specs=in_vmem(2 + len(flat)),
        out_specs=tuple(in_vmem(parts)),
        compiler_params=room(12),
        name="last",
    )(normed, scales, *flat)


def weight_parts(w_gate, w_up, w_down, tp, later_of):
    if tp != 4:
        gate, up, down = (exchange_all(w, "tp") for w in (w_gate, w_up, w_down))
        pairs = [list(pair) for pair in zip(gate, up)]
        return pairs, [[w] for w in down], lambda *parts: list(parts)
    gate1 = swap_with(w_gate, "tp", 1)
    up2 = swap_with(w_up, "tp", 2)
    top = w_gate.shape[0] * 9 // 32
    later_gate, later_up = later_of(w_gate), later_of(w_up)
    up1_top = swap_with(later_up[:top], "tp", 1)
    gate2_top = swap_with(later_gate[:top], "tp", 2)
    up1_low = swap_with(later_up[top:], "tp", 1)
    gate2_low = swap_with(later_gate[top:], "tp", 2)
    up3 = swap_with(up2, "tp", 1)
    gate3 = swap_with(gate1, "tp", 2)
    wide = w_down.shape[1] // 2
    w_late = later_of(w_down)
    left, right = w_late[:, :wide], w_late[:, wide:]
    down1_l = swap_with(left, "tp", 1)
    down2_r = swap_with(right, "tp", 2)
    down1_r = swap_with(right, "tp", 1)
    down2_l = swap_with(left, "tp", 2)
    down3_r = swap_with(down2_r, "tp", 1)
    down3_l = swap_with(down1_l, "tp", 2)
    near = staged(
        [([w_gate], [w_up]), ([gate1], [up1_top, up1_low]), ([gate2_top, gate2_low], [up2])]
    )
    first = [[w] for w in near] + [[gate3, up3]]
    down = [[w_down], [down1_l, down2_r], [down1_r, down2_l], [down3_l, down3_r]]

    def by_distance(own, early, late, last):
        one = jnp.concatenate([early[:, :wide], late[:, :wide]], axis=1)
        two = jnp.concatenate([late[:, wide:], early[:, wide:]], axis=1)
        return [own, one, two, last]

    return first, down, by_distance


def body(
    pool_in,
    doc_ids,
    pool_map,
    pool_scale,
    w_out,
    gate_logit,
    residual,
    first_gain,
    first_bias,
    routes,
    route_weight,
    w_gate,
    w_up,
    w_down,
    second_gain,
    second_bias,
):
    sp, tp = lax.axis_size("sp"), lax.axis_size("tp")
    i, j = lax.axis_index("sp"), lax.axis_index("tp")
    _, positions = pool_in.shape
    quarter = positions // tp

    place = jnp.stack([i, j])
    gains = jnp.stack([first_gain, first_bias, second_gain, second_bias])
    gains = exchange_all(gains, "tp")
    pooled = pooled_channels(pool_in, doc_ids, place)

    def later_of(weight):
        return lax.optimization_barrier((weight, pooled))[0]

    first_w, down_w, by_distance = weight_parts(
        w_gate[0], w_up[0], w_down[0], tp, later_of
    )
    pooled_rel = exchange_all(pooled, "tp")
    my_routes = lax.dynamic_slice_in_dim(routes, j * quarter, quarter, 0)
    my_weights = lax.dynamic_slice_in_dim(route_weight, j * quarter, quarter, 0)
    chosen = jnp.stack([my_routes.astype(F32).T, my_weights.T])
    chosen = jnp.stack([chosen, swap_with(chosen, "sp", 1)])
    chosen = [chosen] + [swap_with(chosen, "sp", 2 * k) for k in range(1, sp // 2)]
    share = token_shares(place, chosen)

    gathered = jnp.concatenate(in_order(pooled_rel, j))
    group_count = gathered.shape[0] // GROUP_W
    grouped = jnp.einsum(
        "gct,gcd->tgd",
        gathered.reshape(group_count, GROUP_W, positions),
        pool_map,
        preferred_element_type=F32,
    )
    mapped = (grouped.reshape(positions, group_count * GROUP_W) * pool_scale).astype(BF16)
    mixer_out = jnp.dot(mapped, w_out, preferred_element_type=F32) * jax.nn.sigmoid(
        gate_logit.astype(F32)
    )
    mixed = ALPHA * residual.astype(F32) + mixer_out

    sent = rows_to_send(place, mixed, tp)
    both = exchange(sent, "tp", 1)
    tokens, normed, scales = first_norm(place, both, gains)

    everyone = line_gather(tokens, "sp")
    inputs, first_hidden = hidden_units(everyone, first_w[0])
    hidden_rel = [first_hidden] + [
        hidden_units([inputs], first_w[k])[1] for k in range(1, tp)
    ]

    groups = []
    half_rows = (sp // 2) * quarter
    for k in range(len(down_w)):
        common = (place, share, hidden_rel, down_w[k])
        other = weighted_outputs(*common, half_rows, half_rows, BF16)
        other = swap_with(other, "sp", 1)
        own = weighted_outputs(*common, 0, half_rows, F32)
        joined = own + other.astype(F32)
        sent = joined.astype(BF16)
        got = exchange(
            [sent[d * quarter : (d + 1) * quarter] for d in range(sp // 2)], "sp", 2
        )
        groups.append([joined[:quarter]] + got[1:])
    out_rel = last_norm(by_distance, normed, scales, groups)
    home_rel = exchange(out_rel, "tp", 1)
    return jnp.concatenate(in_order(home_rel, j))


def solution(mesh):
    return jax.shard_map(
        body,
        mesh=mesh,
        in_specs=(
            P("tp", "sp"),
            P("sp"),
            P(),
            P(),
            P(None, "tp"),
            P("sp", "tp"),
            P("sp", "tp"),
            P("tp"),
            P("tp"),
            P("sp", None),
            P("sp", None),
            P("sp", None, "tp"),
            P("sp", None, "tp"),
            P("sp", None, "tp"),
            P("tp"),
            P("tp"),
        ),
        out_specs=P("sp", "tp"),
        check_vma=False,
    )
```
